512 devices in a mesh: sp: 64 (over z, y), tp: 8 (over x, core).
Axes of the slice: x: 4, y: 8, z: 8, core: 2. Of those that a mesh axis runs over, the one named last changes fastest.
Arguments:
- target: bfloat16 [16384, 1024], P(('sp', 'tp')), may hold values from -60 to 60
- source: bfloat16 [8192, 1024], P('sp'), may hold values from -7 to 7
- target_gains: bfloat16 [2, 4, 1024], replicated, may hold values from 0.099609375 to 1.8984375
- source_gain: bfloat16 [2, 1024], replicated, may hold values from 0.099609375 to 1.8984375
- query_weight: bfloat16 [2, 1024, 1024], P(None, None, 'tp'), may hold values from -0.1875 to 0.1875
- key_weight: bfloat16 [2, 1024, 1024], P(None, None, 'tp'), may hold values from -7.5625 to 7.5625
- value_weight: bfloat16 [2, 1024, 1024], P(None, None, 'tp'), may hold values from -0.1875 to 0.1875
- out_weight: bfloat16 [2, 1024, 1024], P(None, 'tp'), may hold values from -0.1875 to 0.1875
- gate_weight: bfloat16 [2, 1024, 1536], P(None, None, 'tp'), may hold values from -0.1875 to 0.1875
- up_weight: bfloat16 [2, 1024, 1536], P(None, None, 'tp'), may hold values from -0.1875 to 0.1875
- down_weight: bfloat16 [2, 1536, 1024], P(None, 'tp'), may hold values from -0.15625 to 0.15625
Outputs:
- stream: bfloat16 [16384, 1024], P(('sp', 'tp'))
The draws below stay inside these ranges and needn't reach their ends.
All inputs are finite; a program needn't handle non-finite values.
Results may differ from the reference program's by a relative error of at most 0.04.
Values may be sent and summed in bfloat16 or wider, within the bound.
A program may use at most 64 MiB of HBM per device.

```python
import jax
import jax.numpy as jnp
from jax import lax

D = 1024
HEADS = 8
HEAD_DIM = 128
FF = 1536
LAYERS = 2
TGT_DEV = 256
TGT = 16384
SRC = 8192
N_TP = 8


def drawn_rows(key):
    base = jnp.clip(jax.random.normal(jax.random.fold_in(key, 101), (TGT, D), jnp.float32), -6.0, 6.0)
    return base


def draw_target(key, part):
    base = drawn_rows(key)
    return base.astype(jnp.bfloat16)


def draw_source(key, part):
    noise = jnp.clip(jax.random.normal(jax.random.fold_in(key, 105), (SRC, D), jnp.float32), -6.0, 6.0)
    return noise.astype(jnp.bfloat16)


def head_weights(key):
    shape = (LAYERS, D, HEADS * HEAD_DIM)
    first = jnp.clip(jax.random.normal(jax.random.fold_in(key, 201), shape, jnp.float32), -6.0, 6.0) * D ** (-0.5)
    second = jnp.clip(jax.random.normal(jax.random.fold_in(key, 202), shape, jnp.float32), -6.0, 6.0) * D ** (-0.5)
    return (first, second)


def draw_query_weight(key, part):
    first, second = head_weights(key)
    return first.astype(jnp.bfloat16)


def draw_key_weight(key, part):
    first, second = head_weights(key)
    return second.astype(jnp.bfloat16)


def block_scale(stream_key, dims, pieces, smallest, largest):
    loudness = 1.0
    for axis_at, parts in pieces:
        heights = jax.random.uniform(jax.random.fold_in(jax.random.fold_in(stream_key, 6), axis_at), (parts,), jnp.float32, smallest / len(pieces), largest / len(pieces))
        loudness = loudness * jnp.repeat(jnp.exp(heights), dims[axis_at] // parts).reshape((-1,) + (1,) * (len(dims) - 1 - axis_at))
    return loudness


def gaussian(rng, shape, spread, most, pieces=(), kind=jnp.bfloat16):
    values = jax.random.normal(rng, shape, jnp.float32) * spread
    if len(pieces) > 0:
        values = block_scale(rng, shape, pieces, -0.22, 0.18) * values
    return jnp.clip(values, min=-most, max=most).astype(kind)


def setup_inputs(seed: int = 0) -> dict:
    key_list = jax.random.split(jax.random.key(seed), 12)
    target = draw_target(jax.random.fold_in(key_list[11], 71), 0)
    source = draw_source(jax.random.fold_in(key_list[11], 71), 0)
    target_gains = jnp.clip(1.0 + 0.18 * jax.random.normal(key_list[2], (LAYERS, 4, D), jnp.float32), 0.099609375, 1.8984375).astype(jnp.bfloat16)
    source_gain = jnp.clip(1.0 + 0.18 * jax.random.normal(key_list[3], (LAYERS, D), jnp.float32), 0.099609375, 1.8984375).astype(jnp.bfloat16)
    query_weight = draw_query_weight(jax.random.fold_in(key_list[11], 71), 0)
    key_weight = draw_key_weight(jax.random.fold_in(key_list[11], 71), 0)
    value_weight = gaussian(key_list[6], (LAYERS, D, HEADS * HEAD_DIM), D ** -0.5, 0.1875, ((2, 8),))
    out_weight = gaussian(key_list[7], (LAYERS, HEADS * HEAD_DIM, D), (HEADS * HEAD_DIM) ** -0.5, 0.1875, ((1, 8),))
    gate_weight = gaussian(key_list[8], (LAYERS, D, FF), D ** -0.5, 0.1875, ((2, 8),))
    up_weight = gaussian(key_list[9], (LAYERS, D, FF), D ** -0.5, 0.1875, ((2, 8),))
    down_weight = gaussian(key_list[10], (LAYERS, FF, D), FF ** -0.5, 0.15625, ((1, 8),))
    return dict(target=target, source=source, target_gains=target_gains, source_gain=source_gain, query_weight=query_weight, key_weight=key_weight, value_weight=value_weight, out_weight=out_weight, gate_weight=gate_weight, up_weight=up_weight, down_weight=down_weight)


epsilon = 1e-06

def rms_norm(values, gain_row):
    widened = values.astype(jnp.float32)
    inverse = lax.rsqrt(lax.optimization_barrier(jnp.mean(widened * widened, axis=-1, keepdims=True)) + epsilon)
    return widened * inverse * gain_row.astype(jnp.float32)

def blockwise_sum(left, right, pieces_count):
    block_width = left.shape[1] // pieces_count
    summed = jnp.zeros((left.shape[0], right.shape[1]), jnp.float32)
    for index in range(pieces_count):
        partial_value = jnp.dot(left[:, index * block_width:(index + 1) * block_width], right[index * block_width:(index + 1) * block_width], preferred_element_type=jnp.float32)
        summed = summed + lax.optimization_barrier(partial_value.astype(jnp.bfloat16)).astype(jnp.float32)
    return summed.astype(jnp.bfloat16)

def reference(target, source, target_gains, source_gain, query_weight, key_weight, value_weight, out_weight, gate_weight, up_weight, down_weight):
    factor = HEAD_DIM ** (-0.5)
    stream = target
    for layer_index in range(LAYERS):
        layer_gains = target_gains[layer_index]
        normed_source = rms_norm(source, source_gain[layer_index]).astype(jnp.bfloat16)
        key_rows = jnp.dot(normed_source, key_weight[layer_index], preferred_element_type=jnp.float32).astype(jnp.bfloat16)
        value_rows = jnp.dot(normed_source, value_weight[layer_index], preferred_element_type=jnp.float32).astype(jnp.bfloat16)
        key_wide = key_rows.astype(jnp.float32).reshape(SRC, HEADS, HEAD_DIM)
        value_wide = value_rows.astype(jnp.float32).reshape(SRC, HEADS, HEAD_DIM)
        normed = rms_norm(stream, layer_gains[0]).astype(jnp.bfloat16)
        queries = jnp.dot(normed, query_weight[layer_index], preferred_element_type=jnp.float32).astype(jnp.bfloat16)
        query_blocks = queries.astype(jnp.float32).reshape(TGT // TGT_DEV, TGT_DEV, HEADS, HEAD_DIM)

        def attend(query_block):
            scores = jnp.einsum('thd,shd->ths', query_block, key_wide) * factor
            row_max = lax.optimization_barrier(jnp.max(scores, axis=-1, keepdims=True))
            weights = jnp.exp(scores - row_max)
            totals = lax.optimization_barrier(jnp.sum(weights, axis=-1))
            rounded = lax.optimization_barrier(weights.astype(jnp.bfloat16)).astype(jnp.float32)
            blended = jnp.einsum('ths,shd->thd', rounded, value_wide)
            return (blended / totals[..., None]).astype(jnp.bfloat16)
        context = lax.map(attend, query_blocks).reshape(TGT, HEADS * HEAD_DIM)
        attended = blockwise_sum(context, out_weight[layer_index], N_TP)
        stream = (stream.astype(jnp.float32) + rms_norm(attended, layer_gains[1])).astype(jnp.bfloat16)
        mixer_in = rms_norm(stream, layer_gains[2]).astype(jnp.bfloat16)
        gate_part = jnp.dot(mixer_in, gate_weight[layer_index], preferred_element_type=jnp.float32)
        up_part = jnp.dot(mixer_in, up_weight[layer_index], preferred_element_type=jnp.float32)
        hidden = (jax.nn.silu(gate_part) * up_part).astype(jnp.bfloat16)
        mixer_out = blockwise_sum(hidden, down_weight[layer_index], N_TP)
        stream = (stream.astype(jnp.float32) + rms_norm(mixer_out, layer_gains[3])).astype(jnp.bfloat16)
    return stream
```

```python
import functools
import math

import jax
import jax.numpy as jnp
from jax import lax
from jax.experimental import pallas as pl
from jax.experimental.pallas import tpu as pltpu
from jax.sharding import PartitionSpec as P

MESH = pl.DeviceIdType.MESH
BF = jnp.bfloat16
F32 = jnp.float32
EPS = 1e-06
HD = 128
D = 1024
ROWS = 32
GROUP = 128
BLOCKS = 64
LAYERS = 2
STEPS = 8 * LAYERS
QSCALE = HD ** (-0.5) * math.log2(math.e)


def rms(v, gain):
    inverse = lax.rsqrt(jnp.mean(v * v, axis=-1, keepdims=True) + EPS)
    return v * inverse * gain


def dot(a, b):
    return jnp.dot(a, b, preferred_element_type=F32)


def ring_offset(k):
    return ((k + 1) // 2) * (2 * (k % 2) - 1)


def kernel(
    target, source, tgains, sgain, qw_in, kw_in, vw_in, ow_in, gw_in, uw_in, dw_in,
    out,
    src_v, tg_v, sg_v, kw, vw, qw, gw, uw, dw, ow,
    kv, xg, qown, qrecv, qsend, cx, csend, mid, rsend, rs,
    m_ref, l_ref, acc_ref,
    r2, r1, kvs, loc, wts, own_sem, x_recv, x_send, q_recv, q_send, c_recv, c_send, s_recv, s_send,
    pw_recv, pw_send, o_recv, o_send, of_recv, of_send,
):
    sp = lax.axis_index("sp")
    tp = lax.axis_index("tp")
    c = lax.rem(tp, 2)
    x = tp // 2
    z_pos, y_pos = sp // 8, lax.rem(sp, 8)
    f = (1 - c) * y_pos + c * z_pos
    s = (1 - c) * z_pos + c * y_pos

    def sp_of(fp, spos):
        return fp * (1 + 7 * c) + spos * (8 - 7 * c)

    def wrap(v):
        return lax.rem(v + 16, 8)

    ring1 = (sp_of(wrap(f + 1), s), sp_of(wrap(f - 1), s))
    ring2 = (sp_of(f, wrap(s + 1)), sp_of(f, wrap(s - 1)))
    partner = x * 2 + (1 - c)

    def other_x(k):
        return lax.rem(x + k, 4)

    def local(src, dst, sem):
        copy = pltpu.make_async_copy(src, dst, sem)
        copy.start()
        return copy

    first = [
        local(source, src_v, loc.at[0]),
        local(kw_in, kw, loc.at[1]),
        local(vw_in, vw, loc.at[2]),
        local(sgain, sg_v, loc.at[3]),
    ]
    target_load = local(target, xg.at[0, x], loc.at[4])
    gains_load = local(tgains, tg_v, loc.at[5])
    q_load = local(qw_in, qw.at[c], loc.at[6])
    late = [
        local(gw_in, gw.at[c], wts.at[0]),
        local(uw_in, uw.at[c], wts.at[1]),
        local(dw_in, dw.at[c], wts.at[2]),
    ]
    own_rows = pl.ds(pl.multiple_of((c * 4 + x) * HD, HD), HD)
    own_out = [
        local(ow_in.at[l], ow.at[l, own_rows], own_sem.at[l]) for l in range(LAYERS)
    ]

    barrier = pltpu.get_barrier_semaphore()
    peers = [(ring1[0], tp), (ring1[1], tp), (ring2[0], tp), (ring2[1], tp)]
    peers += [(sp, lax.rem(tp + k, 8)) for k in range(1, 8)]
    for peer in peers:
        pl.semaphore_signal(barrier, inc=1, device_id=peer, device_id_type=MESH)
    pl.semaphore_wait(barrier, len(peers))

    def remote(src, dst, send, recv, device):
        pltpu.make_async_remote_copy(
            src_ref=src, dst_ref=dst, send_sem=send, recv_sem=recv,
            device_id=device, device_id_type=MESH,
        ).start()

    def await_bytes(ref, sem):
        pltpu.make_async_copy(ref, ref, sem).wait()

    target_load.wait()
    for k in (2, 1, 3):
        remote(xg.at[0, x], xg.at[0, x], x_send.at[0], x_recv.at[0], (sp, other_x(k) * 2 + c))
    for i, (w_in, buf) in enumerate(((qw_in, qw), (gw_in, gw), (uw_in, uw), (dw_in, dw))):
        remote(w_in, buf.at[c], pw_send.at[i], pw_recv.at[i], (sp, partner))
    for l in range(LAYERS):
        for k in (2, 1, 3):
            remote(
                ow_in.at[l], ow.at[l, own_rows], o_send.at[l], o_recv.at[l],
                (sp, other_x(k) * 2 + c),
            )

    def slot_of(fp, spos):
        return fp * 8 + spos

    for copy in first:
        copy.wait()
    wide = src_v[...].astype(F32)
    scaled = wide * lax.rsqrt(jnp.mean(wide * wide, axis=-1, keepdims=True) + EPS)
    source_gains = sg_v[...].astype(F32)

    def project_source(l):
        normed = (scaled * source_gains[l : l + 1]).astype(BF)
        kv[l, slot_of(f, s), 0] = dot(normed, kw[l]).astype(BF)
        kv[l, slot_of(f, s), 1] = jnp.transpose(dot(normed, vw[l])).astype(BF)

    def send1(l, hop, way):
        delta = hop - 1
        fp = wrap(f - delta) if way == 0 else wrap(f + delta)
        block = kv.at[l, slot_of(fp, s)]
        if hop == 4:
            block = block.at[way]
        remote(block, block, kvs.at[l], r1.at[l, hop - 1, way], (ring1[way], tp))

    def recv1(l, hop, way):
        fp = wrap(f - hop) if way == 0 else wrap(f + hop)
        block = kv.at[l, slot_of(fp, s)]
        if hop == 4:
            block = block.at[way]
        await_bytes(block, r1.at[l, hop - 1, way])

    def send2(n, hop, way):
        l, k = divmod(n, 8)
        fp = wrap(f + ring_offset(k))
        delta = hop - 1
        spos = wrap(s - delta) if way == 0 else wrap(s + delta)
        block = kv.at[l, slot_of(fp, spos)]
        if hop == 4:
            block = block.at[way]
        remote(block, block, kvs.at[l], r2.at[n, hop - 1, way], (ring2[way], tp))

    def recv2(n, hop, way):
        l, k = divmod(n, 8)
        fp = wrap(f + ring_offset(k))
        spos = wrap(s - hop) if way == 0 else wrap(s + hop)
        block = kv.at[l, slot_of(fp, spos)]
        if hop == 4:
            block = block.at[way]
        await_bytes(block, r2.at[n, hop - 1, way])

    def ring_step(m):
        for l in range(LAYERS):
            hop = m - 4 * l
            if hop == 0:
                for way in (0, 1):
                    send1(l, 1, way)
            elif 1 <= hop <= 4:
                for way in (1, 0):
                    recv1(l, hop, way)
                    if hop < 4:
                        send1(l, hop + 1, way)
        if m < STEPS:
            for way in (0, 1):
                send2(m, 1, way)
        for hop in (1, 2, 3, 4):
            n = m - hop
            if 0 <= n < STEPS:
                for way in (0, 1):
                    recv2(n, hop, way)
                    if hop < 4:
                        send2(n, hop + 1, way)

    def attend(m, l):
        low = max(1, m - (8 * l + 7))
        high = min(4, m - 8 * l)
        if low > high:
            return

        def body(hop, carry):
            k = m - hop - 8 * l
            fp = wrap(f + ring_offset(k))
            left = slot_of(fp, wrap(s - lax.rem(hop, 4)))
            right = slot_of(fp, wrap(s + hop))
            queries = qcat(l)
            key_pair = jnp.concatenate([kv[l, left, 0], kv[l, right, 0]], axis=0)
            value_pair = jnp.concatenate([kv[l, left, 1], kv[l, right, 1]], axis=1)
            scores = dot(key_pair, queries)
            old = m_ref[...]
            new = jnp.maximum(old, jnp.max(scores, axis=0, keepdims=True))
            shrink = jnp.exp2(old - new)
            weights = jnp.exp2(scores - new)
            m_ref[...] = new
            l_ref[...] = l_ref[...] * shrink + jnp.sum(weights, axis=0, keepdims=True)
            acc_ref[...] = acc_ref[...] * shrink + dot(value_pair, weights.astype(BF))
            return carry

        lax.fori_loop(low, high + 1, body, 0)

    def qcat(l):
        return jnp.concatenate([qown[l], qrecv[l]], axis=1)

    def start_queries(l):
        gain = tg_v[l].astype(F32)[0:1]
        rows = xg[l].reshape(GROUP, D).astype(F32)
        normed = rms(rows, gain).astype(BF)
        theirs = dot(normed, qw[1 - c, l]) * QSCALE
        qsend[l] = jnp.transpose(theirs).astype(BF)
        remote(qsend.at[l], qrecv.at[l], q_send.at[l], q_recv.at[l], (sp, partner))
        mine = dot(normed, qw[c, l]) * QSCALE
        qown[l] = jnp.transpose(mine).astype(BF)
        m_ref[...] = jnp.full_like(m_ref, -1e30)
        l_ref[...] = jnp.zeros_like(l_ref)
        acc_ref[...] = jnp.zeros_like(acc_ref)

    def await_queries(l):
        await_bytes(qrecv.at[l], q_recv.at[l])

    def send_context(l):
        context = jnp.transpose(acc_ref[...] / l_ref[...]).astype(BF)
        slot = c * 4 + x
        csend[l] = context
        for k in (2, 1, 3):
            remote(
                csend.at[l, pl.ds(0, GROUP)], cx.at[l, slot], c_send.at[l], c_recv.at[l],
                (sp, other_x(k) * 2 + c),
            )
            remote(
                csend.at[l, pl.ds(GROUP, GROUP)], cx.at[l, slot], c_send.at[l], c_recv.at[l],
                (sp, other_x(k) * 2 + 1 - c),
            )
        remote(
            csend.at[l, pl.ds(GROUP, GROUP)], cx.at[l, slot], c_send.at[l], c_recv.at[l],
            (sp, partner),
        )
        cx[l, slot] = context[:GROUP]

    def after_context(l):
        await_bytes(cx.at[l, pl.ds(0, 7)], c_recv.at[l])
        gains = tg_v[l].astype(F32)
        contexts = jnp.concatenate([cx[l, j] for j in range(8)], axis=1)
        attended = dot(contexts, ow[l]).astype(BF).astype(F32)
        rows = xg[l].reshape(GROUP, D).astype(F32)
        stream = (rows + rms(attended, gains[1:2])).astype(BF)
        mid[l] = stream
        mixer_in = rms(stream.astype(F32), gains[2:3]).astype(BF)
        mixed = None
        for j in range(2):
            gate = dot(mixer_in, gw[j, l])
            up = dot(mixer_in, uw[j, l])
            hidden = (gate / (1.0 + jnp.exp(-gate)) * up).astype(BF)
            term = dot(hidden, dw[j, l])
            mixed = term if mixed is None else mixed + term
        rsend[l] = mixed.astype(BF).reshape(4, ROWS, D)
        for k in (2, 1, 3):
            remote(
                rsend.at[l, other_x(k)], rs.at[l, x], s_send.at[l], s_recv.at[l],
                (sp, other_x(k) * 2 + c),
            )
        rs[l, x] = rsend[l, x]

    def after_sum(l):
        await_bytes(rs.at[l, pl.ds(0, 3)], s_recv.at[l])
        gain = tg_v[l].astype(F32)[3:4]
        total = rs[l, 0].astype(F32)
        for j in range(1, 4):
            total = total + rs[l, j].astype(F32)
        mixer_out = total.astype(BF).astype(F32)
        own = mid[l, pl.ds(pl.multiple_of(x * ROWS, ROWS), ROWS)].astype(F32)
        return (own + rms(mixer_out, gain)).astype(BF)

    def forward_out(l):
        for k in range(1):
            own_out[l].wait()
        await_bytes(ow.at[l, pl.ds(0, 3 * HD)], o_recv.at[l])
        plane = pl.ds(pl.multiple_of(c * 512, 512), 512)
        remote(ow.at[l, plane], ow.at[l, plane], of_send.at[l], of_recv.at[l], (sp, partner))

    project_source(0)
    ring_step(0)
    project_source(1)
    ring_step(1)
    ring_step(2)
    gains_load.wait()
    q_load.wait()
    await_bytes(qw.at[0], pw_recv.at[0])
    await_bytes(xg.at[0, pl.ds(0, 3)], x_recv.at[0])
    start_queries(0)
    ring_step(3)
    await_queries(0)
    for m in range(1, 4):
        attend(m, 0)
    for m in range(4, 12):
        ring_step(m)
        if m == 7:
            forward_out(0)
        if m == 10:
            forward_out(1)
        attend(m, 0)
    send_context(0)
    ring_step(12)
    ring_step(13)
    for copy in late:
        copy.wait()
    for i, buf in enumerate((gw, uw, dw)):
        await_bytes(buf.at[0], pw_recv.at[1 + i])
    await_bytes(ow.at[0, pl.ds(0, 512)], of_recv.at[0])
    after_context(0)
    ring_step(14)
    ring_step(15)
    own = after_sum(0)
    xg[1, x] = own
    for k in (2, 1, 3):
        remote(xg.at[1, x], xg.at[1, x], x_send.at[1], x_recv.at[1], (sp, other_x(k) * 2 + c))
    ring_step(16)
    ring_step(17)
    await_bytes(xg.at[1, pl.ds(0, 3)], x_recv.at[1])
    start_queries(1)
    ring_step(18)
    await_queries(1)
    for m in range(9, 19):
        attend(m, 1)
    ring_step(19)
    attend(19, 1)
    send_context(1)
    await_bytes(ow.at[1, pl.ds(0, 512)], of_recv.at[1])
    after_context(1)
    out[...] = after_sum(1)

    for l in range(LAYERS):
        await_bytes(kv.at[l, pl.ds(0, 63)], kvs.at[l])
        await_bytes(xg.at[l, pl.ds(0, 3)], x_send.at[l])
        await_bytes(qsend.at[l], q_send.at[l])
        await_bytes(cx.at[l, pl.ds(0, 7)], c_send.at[l])
        await_bytes(rs.at[l, pl.ds(0, 3)], s_send.at[l])
        await_bytes(ow.at[l, pl.ds(0, 3 * HD)], o_send.at[l])
        await_bytes(ow.at[l, pl.ds(0, 512)], of_send.at[l])
    for i, buf in enumerate((qw, gw, uw, dw)):
        await_bytes(buf.at[0], pw_send.at[i])


def per_device(*args):
    ff = args[8].shape[2]
    hbm = pl.BlockSpec(memory_space=pl.ANY)
    vmem = pltpu.VMEM
    dma = pltpu.SemaphoreType.DMA
    scratch = [
        vmem((128, D), BF),
        vmem((LAYERS, 4, D), BF),
        vmem((LAYERS, D), BF),
        vmem((LAYERS, D, HD), BF),
        vmem((LAYERS, D, HD), BF),
        vmem((2, LAYERS, D, HD), BF),
        vmem((2, LAYERS, D, ff), BF),
        vmem((2, LAYERS, D, ff), BF),
        vmem((2, LAYERS, ff, D), BF),
        vmem((LAYERS, D, D), BF),
        vmem((LAYERS, BLOCKS, 2, HD, HD), BF),
        vmem((LAYERS, 4, ROWS, D), BF),
        vmem((LAYERS, HD, GROUP), BF),
        vmem((LAYERS, HD, GROUP), BF),
        vmem((LAYERS, HD, GROUP), BF),
        vmem((LAYERS, 8, GROUP, HD), BF),
        vmem((LAYERS, 2 * GROUP, HD), BF),
        vmem((LAYERS, GROUP, D), BF),
        vmem((LAYERS, 4, ROWS, D), BF),
        vmem((LAYERS, 4, ROWS, D), BF),
        vmem((1, 2 * GROUP), F32),
        vmem((1, 2 * GROUP), F32),
        vmem((HD, 2 * GROUP), F32),
        dma((STEPS, 4, 2)),
        dma((LAYERS, 4, 2)),
        dma((LAYERS,)),
        dma((7,)),
        dma((3,)),
        dma((LAYERS,)),
    ]
    scratch += [dma((LAYERS,)) for _ in range(8)]
    scratch += [dma((4,)), dma((4,))]
    scratch += [dma((LAYERS,)) for _ in range(4)]
    return pl.pallas_call(
        kernel,
        out_shape=jax.ShapeDtypeStruct((ROWS, D), BF),
        in_specs=[hbm] * 11,
        out_specs=pl.BlockSpec(memory_space=pltpu.VMEM),
        scratch_shapes=scratch,
        compiler_params=pltpu.CompilerParams(
            collective_id=0, has_side_effects=True, vmem_limit_bytes=60 * 1024 * 1024
        ),
    )(*args)


def solution(mesh):
    placed = (
        P(("sp", "tp"), None),
        P("sp", None),
        P(),
        P(),
        P(None, None, "tp"),
        P(None, None, "tp"),
        P(None, None, "tp"),
        P(None, "tp", None),
        P(None, None, "tp"),
        P(None, None, "tp"),
        P(None, "tp", None),
    )
    return jax.shard_map(
        per_device, mesh=mesh, in_specs=placed, out_specs=P(("sp", "tp"), None), check_vma=False
    )
```

```python
import functools
import math

import jax
import jax.numpy as jnp
from jax import lax
from jax.experimental import pallas as pl
from jax.experimental.pallas import tpu as pltpu
from jax.sharding import PartitionSpec as P

MESH = pl.DeviceIdType.MESH
BF = jnp.bfloat16
F32 = jnp.float32
EPS = 1e-06
HD = 128
D = 1024
ROWS = 32
GROUP = 128
BLOCKS = 64
LAYERS = 2
STEPS = 8 * LAYERS
LATENCY = 2.5
SECOND_START = 25.0
QSCALE = HD ** (-0.5) * math.log2(math.e)


def rms(v, gain):
    inverse = lax.rsqrt(jnp.mean(v * v, axis=-1, keepdims=True) + EPS)
    return v * inverse * gain


def dot(a, b):
    return jnp.dot(a, b, preferred_element_type=F32)


def ring_offset(k):
    return ((k + 1) // 2) * (2 * (k % 2) - 1)


def ring_events(latency, second_start, block=0.7):
    queues = {(way, ring): [] for way in (0, 1) for ring in (1, 2)}
    flying, events = [], []
    starts = [(0.0, 0), (second_start, 1)]
    halves = [0, 0]
    now = 0.0

    def put(ring, index, hop, way):
        size = block if hop < 4 else block / 2
        queues[way, ring].append([size, (ring, index, hop, way)])

    def fresh(n):
        put(2, n, 1, 0)
        put(2, n, 1, 1)

    while True:
        times = [t for t, _ in starts] + [t for t, _ in flying]
        for way in (0, 1):
            busy = [r for r in (1, 2) if queues[way, r]]
            times += [now + queues[way, r][0][0] * len(busy) for r in busy]
        if not times:
            return events
        step = min(times) - now
        for way in (0, 1):
            busy = [r for r in (1, 2) if queues[way, r]]
            for r in busy:
                queues[way, r][0][0] -= step / len(busy)
        now += step
        for pair in sorted(queues):
            if queues[pair] and queues[pair][0][0] < 1e-9:
                flying.append((now + latency, queues[pair].pop(0)[1]))
        for start in [v for v in starts if v[0] <= now + 1e-9]:
            starts.remove(start)
            events.append((now, (0, start[1], 0, 0)))
            put(1, start[1], 1, 0)
            put(1, start[1], 1, 1)
            fresh(8 * start[1])
        for arrival in [v for v in flying if v[0] <= now + 1e-9]:
            flying.remove(arrival)
            events.append((now, arrival[1]))
            ring, index, hop, way = arrival[1]
            if hop < 4:
                put(ring, index, hop + 1, way)
            if ring == 1:
                if hop < 4:
                    fresh(8 * index + 2 * hop - way)
                else:
                    halves[index] += 1
                    if halves[index] == 2:
                        fresh(8 * index + 7)


def kernel(
    target, source, tgains, sgain, qw_in, kw_in, vw_in, ow_in, gw_in, uw_in, dw_in,
    out,
    src_v, tg_v, sg_v, kw, vw, qw, gu, dn, ow,
    kv, xg, qown, qrecv, qsend, cx, csend, mid, rsend, rs,
    m_ref, l_ref, acc_ref, scores_ref,
    r2, r1, kvs, loc, wts, own_sem, x_recv, x_send, q_recv, q_send, c_recv, c_send, s_recv, s_send,
    pw_recv, pw_send, o_recv, o_send, of_recv, of_send,
):
    sp = lax.axis_index("sp")
    tp = lax.axis_index("tp")
    c = lax.rem(tp, 2)
    x = tp // 2
    z_pos, y_pos = sp // 8, lax.rem(sp, 8)
    f = (1 - c) * y_pos + c * z_pos
    s = (1 - c) * z_pos + c * y_pos

    def sp_of(fp, spos):
        return fp * (1 + 7 * c) + spos * (8 - 7 * c)

    def wrap(v):
        return lax.rem(v + 16, 8)

    ring1 = (sp_of(wrap(f + 1), s), sp_of(wrap(f - 1), s))
    ring2 = (sp_of(f, wrap(s + 1)), sp_of(f, wrap(s - 1)))
    partner = x * 2 + (1 - c)

    def other_x(k):
        return lax.rem(x + k, 4)

    def local(src, dst, sem):
        copy = pltpu.make_async_copy(src, dst, sem)
        copy.start()
        return copy

    first = [
        local(source, src_v, loc.at[0]),
        local(kw_in, kw, loc.at[1]),
        local(vw_in, vw, loc.at[2]),
        local(sgain, sg_v, loc.at[3]),
    ]
    target_load = local(target, xg.at[0, x], loc.at[4])
    gains_load = local(tgains, tg_v, loc.at[5])
    q_load = local(qw_in, qw.at[c], loc.at[6])
    ff = dw_in.shape[1]
    gate_part = gu.at[:, pl.ds(pl.multiple_of(c * 2 * ff, 2 * ff), ff)]
    up_part = gu.at[:, pl.ds(pl.multiple_of(c * 2 * ff + ff, ff), ff)]
    down_part = dn.at[:, pl.ds(pl.multiple_of(c * ff, ff), ff)]
    late = [
        local(gw_in, gate_part, wts.at[0]),
        local(uw_in, up_part, wts.at[1]),
        local(dw_in, down_part, wts.at[2]),
    ]
    own_rows = pl.ds(pl.multiple_of((c * 4 + x) * HD, HD), HD)
    own_out = [
        local(ow_in.at[l], ow.at[l, own_rows], own_sem.at[l]) for l in range(LAYERS)
    ]

    def remote(src, dst, send, recv, device):
        pltpu.make_async_remote_copy(
            src_ref=src, dst_ref=dst, send_sem=send, recv_sem=recv,
            device_id=device, device_id_type=MESH,
        ).start()

    def await_bytes(ref, sem):
        pltpu.make_async_copy(ref, ref, sem).wait()

    def slot_of(fp, spos):
        return fp * 8 + spos

    for copy in first:
        copy.wait()
    wide = src_v[...].astype(F32)
    scaled = wide * lax.rsqrt(jnp.mean(wide * wide, axis=-1, keepdims=True) + EPS)
    source_gains = sg_v[...].astype(F32)

    def project_source(l):
        normed = (scaled * source_gains[l : l + 1]).astype(BF)
        kv[l, slot_of(f, s), 0] = dot(normed, kw[l]).astype(BF)
        kv[l, slot_of(f, s), 1] = jnp.transpose(dot(normed, vw[l])).astype(BF)

    def send1(l, hop, way):
        delta = hop - 1
        fp = wrap(f - delta) if way == 0 else wrap(f + delta)
        block = kv.at[l, slot_of(fp, s)]
        if hop == 4:
            block = block.at[way]
        remote(block, block, kvs.at[l], r1.at[l, hop - 1, way], (ring1[way], tp))

    def recv1(l, hop, way):
        fp = wrap(f - hop) if way == 0 else wrap(f + hop)
        block = kv.at[l, slot_of(fp, s)]
        if hop == 4:
            block = block.at[way]
        await_bytes(block, r1.at[l, hop - 1, way])

    def send2(n, hop, way):
        l, k = divmod(n, 8)
        fp = wrap(f + ring_offset(k))
        delta = hop - 1
        spos = wrap(s - delta) if way == 0 else wrap(s + delta)
        block = kv.at[l, slot_of(fp, spos)]
        if hop == 4:
            block = block.at[way]
        remote(block, block, kvs.at[l], r2.at[n, hop - 1, way], (ring2[way], tp))

    def recv2(n, hop, way):
        l, k = divmod(n, 8)
        fp = wrap(f + ring_offset(k))
        spos = wrap(s - hop) if way == 0 else wrap(s + hop)
        block = kv.at[l, slot_of(fp, spos)]
        if hop == 4:
            block = block.at[way]
        await_bytes(block, r2.at[n, hop - 1, way])

    halves = {}
    waiting = []

    def handle(event):
        ring, index, hop, way = event
        if ring == 0:
            for w in (0, 1):
                send1(index, 1, w)
            for w in (0, 1):
                send2(8 * index, 1, w)
            waiting.append((index, 0, 0))
            return
        if hop == 4:
            halves[ring, index] = halves.get((ring, index), 0) + 1
        whole = hop < 4 or halves[ring, index] == 2
        if ring == 1:
            k = 2 * hop - way if hop < 4 else 7
            recv1(index, hop, way)
            if hop < 4:
                send1(index, hop + 1, way)
            if whole:
                for w in (0, 1):
                    send2(8 * index + k, 1, w)
                waiting.append((index, k, 0))
        else:
            recv2(index, hop, way)
            if hop < 4:
                send2(index, hop + 1, way)
            if whole:
                waiting.append((index // 8, index % 8, -hop if way == 0 else hop))

    groups = {0: [], 1: []}

    def attend(l, slots):
        done = groups[l]
        if slots is not None:
            keys = jnp.concatenate([kv[l, slot, 0] for slot in slots], axis=0)
            scores_ref[len(done) % 2] = dot(keys, qcat(l))
            done.append(slots)
        if len(done) == 1 and slots is not None:
            return
        past = -2 if slots is not None else -1
        values = jnp.concatenate([kv[l, slot, 1] for slot in done[past]], axis=1)
        scores = scores_ref[(len(done) + past) % 2]
        old = m_ref[...]
        new = jnp.maximum(old, jnp.max(scores, axis=0, keepdims=True))
        shrink = jnp.exp2(old - new)
        weights = jnp.exp2(scores - new)
        m_ref[...] = new
        l_ref[...] = l_ref[...] * shrink + jnp.sum(weights, axis=0, keepdims=True)
        acc_ref[...] = acc_ref[...] * shrink + dot(values, weights.astype(BF))

    def attend_waiting(l):
        blocks = [v for v in waiting if v[0] == l][:8]
        for v in blocks:
            waiting.remove(v)
        attend(l, [slot_of(wrap(f + ring_offset(k)), wrap(s + d)) for _, k, d in blocks])

    def qcat(l):
        return jnp.concatenate([qown[l], qrecv[l]], axis=1)

    def start_queries(l):
        gain = tg_v[l].astype(F32)[0:1]
        rows = xg[l].reshape(GROUP, D).astype(F32)
        normed = rms(rows, gain).astype(BF)
        theirs = dot(normed, qw[1 - c, l]) * QSCALE
        qsend[l] = jnp.transpose(theirs).astype(BF)
        remote(qsend.at[l], qrecv.at[l], q_send.at[l], q_recv.at[l], (sp, partner))
        mine = dot(normed, qw[c, l]) * QSCALE
        qown[l] = jnp.transpose(mine).astype(BF)
        m_ref[...] = jnp.full_like(m_ref, -1e30)
        l_ref[...] = jnp.zeros_like(l_ref)
        acc_ref[...] = jnp.zeros_like(acc_ref)

    def await_queries(l):
        await_bytes(qrecv.at[l], q_recv.at[l])

    def send_context(l):
        context = jnp.transpose(acc_ref[...] / l_ref[...]).astype(BF)
        slot = c * 4 + x
        csend[l] = context
        for k in (2, 1, 3):
            remote(
                csend.at[l, pl.ds(0, GROUP)], cx.at[l, slot], c_send.at[l], c_recv.at[l],
                (sp, other_x(k) * 2 + c),
            )
            remote(
                csend.at[l, pl.ds(GROUP, GROUP)], cx.at[l, slot], c_send.at[l], c_recv.at[l],
                (sp, other_x(k) * 2 + 1 - c),
            )
        remote(
            csend.at[l, pl.ds(GROUP, GROUP)], cx.at[l, slot], c_send.at[l], c_recv.at[l],
            (sp, partner),
        )
        cx[l, slot] = context[:GROUP]

    def after_context(l, between=None):
        await_bytes(cx.at[l, pl.ds(0, 7)], c_recv.at[l])
        gains = tg_v[l].astype(F32)
        contexts = jnp.concatenate([cx[l, j] for j in range(8)], axis=1)
        attended = dot(contexts, ow[l]).astype(BF).astype(F32)
        rows = xg[l].reshape(GROUP, D).astype(F32)
        stream = (rows + rms(attended, gains[1:2])).astype(BF)
        mid[l] = stream
        if between is not None:
            between()
        mixer_in = rms(mid[l].astype(F32), gains[2:3]).astype(BF)
        both = lax.dot_general(
            gu[l], mixer_in, (((1,), (1,)), ((), ())), preferred_element_type=F32
        )
        parts = []
        for j in range(2):
            gate = both[2 * j * ff : (2 * j + 1) * ff]
            up = both[(2 * j + 1) * ff : (2 * j + 2) * ff]
            parts.append(gate / (1.0 + jnp.exp(-gate)) * up)
        hidden = jnp.transpose(jnp.concatenate(parts, axis=0)).astype(BF)
        mixed = dot(hidden, dn[l])
        rsend[l] = mixed.astype(BF).reshape(4, ROWS, D)
        for k in (2, 1, 3):
            remote(
                rsend.at[l, other_x(k)], rs.at[l, x], s_send.at[l], s_recv.at[l],
                (sp, other_x(k) * 2 + c),
            )
        rs[l, x] = rsend[l, x]

    def after_sum(l):
        await_bytes(rs.at[l, pl.ds(0, 3)], s_recv.at[l])
        gain = tg_v[l].astype(F32)[3:4]
        total = rs[l, 0].astype(F32)
        for j in range(1, 4):
            total = total + rs[l, j].astype(F32)
        mixer_out = total.astype(BF).astype(F32)
        own = mid[l, pl.ds(pl.multiple_of(x * ROWS, ROWS), ROWS)].astype(F32)
        return own + rms(mixer_out, gain)

    def forward_out(l):
        own_out[l].wait()
        await_bytes(ow.at[l, pl.ds(0, 3 * HD)], o_recv.at[l])
        plane = pl.ds(pl.multiple_of(c * 512, 512), 512)
        remote(ow.at[l, plane], ow.at[l, plane], of_send.at[l], of_recv.at[l], (sp, partner))

    def send_target():
        target_load.wait()
        for k in (2, 1, 3):
            remote(xg.at[0, x], xg.at[0, x], x_send.at[0], x_recv.at[0], (sp, other_x(k) * 2 + c))
        remote(qw_in, qw.at[c], pw_send.at[0], pw_recv.at[0], (sp, partner))

    def send_out(l):
        for k in (2, 1, 3):
            remote(
                ow_in.at[l], ow.at[l, own_rows], o_send.at[l], o_recv.at[l],
                (sp, other_x(k) * 2 + c),
            )

    def send_ff():
        for i, (w_in, part) in enumerate(((gw_in, gate_part), (uw_in, up_part), (dw_in, down_part))):
            remote(w_in, part, pw_send.at[1 + i], pw_recv.at[1 + i], (sp, partner))

    project_source(0)
    barrier = pltpu.get_barrier_semaphore()
    peers = [(ring1[0], tp), (ring1[1], tp), (ring2[0], tp), (ring2[1], tp)]
    peers += [(sp, lax.rem(tp + k, 8)) for k in range(1, 8)]
    for peer in peers:
        pl.semaphore_signal(barrier, inc=1, device_id=peer, device_id_type=MESH)
    pl.semaphore_wait(barrier, len(peers))

    events = ring_events(LATENCY, SECOND_START)
    last_first = max(t for t, (r, i, _, _) in events if i < (8 if r == 2 else 1))
    hooks = {}

    def run_until(limit, attending):
        while events and events[0][0] <= limit:
            when, event = events.pop(0)
            for hook_time in sorted(hooks):
                if hook_time <= when:
                    hooks.pop(hook_time)()
            handle(event)
            if attending is not None and sum(v[0] == attending for v in waiting) >= 8:
                attend_waiting(attending)

    hooks[20.0] = lambda: forward_out(0)
    hooks[29.0] = lambda: forward_out(1)
    run_until(0.0, None)
    send_target()
    project_source(1)
    send_out(0)
    run_until(6.0, None)
    send_out(1)
    gains_load.wait()
    q_load.wait()
    await_bytes(qw.at[0], pw_recv.at[0])
    await_bytes(xg.at[0, pl.ds(0, 3)], x_recv.at[0])
    start_queries(0)
    run_until(9.0, None)
    send_ff()
    await_queries(0)
    run_until(last_first, 0)
    attend(0, None)
    send_context(0)
    run_until(last_first + 6.5, None)
    for copy in late:
        copy.wait()
    for i, part in enumerate((gate_part, up_part, down_part)):
        await_bytes(part, pw_recv.at[1 + i])
    await_bytes(ow.at[0, pl.ds(0, 512)], of_recv.at[0])
    after_context(0, lambda: run_until(last_first + 7.7, None))
    run_until(last_first + 13.5, None)
    xg[1, x] = after_sum(0).astype(BF)
    for k in (2, 1, 3):
        remote(xg.at[1, x], xg.at[1, x], x_send.at[1], x_recv.at[1], (sp, other_x(k) * 2 + c))
    run_until(last_first + 18.5, None)
    await_bytes(xg.at[1, pl.ds(0, 3)], x_recv.at[1])
    start_queries(1)
    run_until(last_first + 20.5, None)
    await_queries(1)
    while sum(v[0] == 1 for v in waiting) >= 8:
        attend_waiting(1)
    run_until(1000.0, 1)
    attend(1, None)
    send_context(1)
    await_bytes(ow.at[1, pl.ds(0, 512)], of_recv.at[1])
    after_context(1)
    out[...] = after_sum(1)

    for l in range(LAYERS):
        await_bytes(kv.at[l, pl.ds(0, 63)], kvs.at[l])
        await_bytes(xg.at[l, pl.ds(0, 3)], x_send.at[l])
        await_bytes(qsend.at[l], q_send.at[l])
        await_bytes(cx.at[l, pl.ds(0, 7)], c_send.at[l])
        await_bytes(rs.at[l, pl.ds(0, 3)], s_send.at[l])
        await_bytes(ow.at[l, pl.ds(0, 3 * HD)], o_send.at[l])
        await_bytes(ow.at[l, pl.ds(0, 512)], of_send.at[l])
    await_bytes(qw.at[0], pw_send.at[0])
    for i, part in enumerate((gate_part, up_part, down_part)):
        await_bytes(part, pw_send.at[1 + i])


def per_device(*args):
    args = list(args)
    ff = args[8].shape[2]
    args[8] = jnp.swapaxes(args[8], 1, 2)
    args[9] = jnp.swapaxes(args[9], 1, 2)
    hbm = pl.BlockSpec(memory_space=pl.ANY)
    vmem = pltpu.VMEM
    dma = pltpu.SemaphoreType.DMA
    scratch = [
        vmem((128, D), BF),
        vmem((LAYERS, 4, D), BF),
        vmem((LAYERS, D), BF),
        vmem((LAYERS, D, HD), BF),
        vmem((LAYERS, D, HD), BF),
        vmem((2, LAYERS, D, HD), BF),
        vmem((LAYERS, 4 * ff, D), BF),
        vmem((LAYERS, 2 * ff, D), BF),
        vmem((LAYERS, D, D), BF),
        vmem((LAYERS, BLOCKS, 2, HD, HD), BF),
        vmem((LAYERS, 4, ROWS, D), BF),
        vmem((LAYERS, HD, GROUP), BF),
        vmem((LAYERS, HD, GROUP), BF),
        vmem((LAYERS, HD, GROUP), BF),
        vmem((LAYERS, 8, GROUP, HD), BF),
        vmem((LAYERS, 2 * GROUP, HD), BF),
        vmem((LAYERS, GROUP, D), BF),
        vmem((LAYERS, 4, ROWS, D), BF),
        vmem((LAYERS, 4, ROWS, D), BF),
        vmem((1, 2 * GROUP), F32),
        vmem((1, 2 * GROUP), F32),
        vmem((HD, 2 * GROUP), F32),
        vmem((2, 8 * HD, 2 * GROUP), F32),
        dma((STEPS, 4, 2)),
        dma((LAYERS, 4, 2)),
        dma((LAYERS,)),
        dma((7,)),
        dma((3,)),
        dma((LAYERS,)),
    ]
    scratch += [dma((LAYERS,)) for _ in range(8)]
    scratch += [dma((4,)), dma((4,))]
    scratch += [dma((LAYERS,)) for _ in range(4)]
    wide = pl.pallas_call(
        kernel,
        out_shape=jax.ShapeDtypeStruct((ROWS, D), F32),
        in_specs=[hbm] * 11,
        out_specs=pl.BlockSpec(memory_space=pltpu.VMEM),
        scratch_shapes=scratch,
        compiler_params=pltpu.CompilerParams(
            collective_id=0, has_side_effects=True, vmem_limit_bytes=60 * 1024 * 1024
        ),
    )(*args)
    return wide.astype(BF)


def solution(mesh):
    placed = (
        P(("sp", "tp"), None),
        P("sp", None),
        P(),
        P(),
        P(None, None, "tp"),
        P(None, None, "tp"),
        P(None, None, "tp"),
        P(None, "tp", None),
        P(None, None, "tp"),
        P(None, None, "tp"),
        P(None, "tp", None),
    )
    return jax.shard_map(
        per_device, mesh=mesh, in_specs=placed, out_specs=P(("sp", "tp"), None), check_vma=False
    )
```

```python
import functools
import math

import jax
import jax.numpy as jnp
from jax import lax
from jax.experimental import pallas as pl
from jax.experimental.pallas import tpu as pltpu
from jax.sharding import PartitionSpec as P

MESH = pl.DeviceIdType.MESH
BF = jnp.bfloat16
F32 = jnp.float32
EPS = 1e-06
HD = 128
D = 1024
ROWS = 32
GROUP = 128
HALF = ROWS // 2
PART = GROUP // 2
BLOCKS = 64
LAYERS = 2
STEPS = 8 * LAYERS
LATENCY = 2.5
SECOND_START = 1.0
RELEASES = [26.0 + 1.4 * j for j in range(8)]
MARKS = (3.5, 5.0, 9.0, 14.0, 15.5)
QSCALE = HD ** (-0.5) * math.log2(math.e)


def rms(v, gain):
    inverse = lax.rsqrt(jnp.mean(v * v, axis=-1, keepdims=True) + EPS)
    return v * inverse * gain


def dot(a, b):
    return jnp.dot(a, b, preferred_element_type=F32)


def ring_offset(k):
    return ((k + 1) // 2) * (2 * (k % 2) - 1)


def ring_events(latency, second_start, releases, block=0.7):
    queues = {(way, ring): [] for way in (0, 1) for ring in (1, 2)}
    flying, events = [], []
    starts = [(0.0, (0, 0, 0, 0)), (second_start, (0, 1, 0, 0))]
    starts += [(t, (3, 8 + j, 0, 0)) for j, t in enumerate(releases)]
    halves = [0, 0]
    here, released = set(), set()
    now = 0.0

    def put(ring, index, hop, way):
        size = block if hop < 4 else block / 2
        queues[way, ring].append([size, (ring, index, hop, way)])

    def fresh(n):
        if n < 8 or (n in here and n in released):
            put(2, n, 1, 0)
            put(2, n, 1, 1)

    def arrived(n):
        here.add(n)
        fresh(n)

    while True:
        times = [t for t, _ in starts] + [t for t, _ in flying]
        for way in (0, 1):
            busy = [r for r in (1, 2) if queues[way, r]]
            times += [now + queues[way, r][0][0] * len(busy) for r in busy]
        if not times:
            return events
        step = min(times) - now
        for way in (0, 1):
            busy = [r for r in (1, 2) if queues[way, r]]
            for r in busy:
                queues[way, r][0][0] -= step / len(busy)
        now += step
        for pair in sorted(queues):
            if queues[pair] and queues[pair][0][0] < 1e-9:
                flying.append((now + latency, queues[pair].pop(0)[1]))
        for start in [v for v in starts if v[0] <= now + 1e-9]:
            starts.remove(start)
            events.append((now, start[1]))
            kind, index, _, _ = start[1]
            if kind == 0:
                put(1, index, 1, 0)
                put(1, index, 1, 1)
                arrived(8 * index)
            else:
                released.add(index)
                fresh(index)
        for arrival in [v for v in flying if v[0] <= now + 1e-9]:
            flying.remove(arrival)
            events.append((now, arrival[1]))
            ring, index, hop, way = arrival[1]
            if hop < 4:
                put(ring, index, hop + 1, way)
            if ring == 1:
                if hop < 4:
                    arrived(8 * index + 2 * hop - way)
                else:
                    halves[index] += 1
                    if halves[index] == 2:
                        arrived(8 * index + 7)


def kernel(
    target, source, tgains, sgain, qw_in, kw_in, vw_in, ow_in, gw_in, uw_in, dw_in,
    out,
    src_v, tg_v, sg_v, kw, vw, qw, raw, gu, dn, ow,
    kv, xg, qown, qrecv, qsend, cx, csend, mid, rsend, rs,
    m_ref, l_ref, acc_ref, scores_ref,
    r2, r1, kvs, loc, wts, own_sem, x_recv, x_send, q_recv, q_send, c_recv, c_send, s_recv, s_send,
    pw_recv, pw_send, o_recv, o_send, of_recv, of_send,
):
    sp = lax.axis_index("sp")
    tp = lax.axis_index("tp")
    c = lax.rem(tp, 2)
    x = tp // 2
    z_pos, y_pos = sp // 8, lax.rem(sp, 8)
    f = (1 - c) * y_pos + c * z_pos
    s = (1 - c) * z_pos + c * y_pos

    def sp_of(fp, spos):
        return fp * (1 + 7 * c) + spos * (8 - 7 * c)

    def wrap(v):
        return lax.rem(v + 16, 8)

    ring1 = (sp_of(wrap(f + 1), s), sp_of(wrap(f - 1), s))
    ring2 = (sp_of(f, wrap(s + 1)), sp_of(f, wrap(s - 1)))
    partner = x * 2 + (1 - c)

    def other_x(k):
        return lax.rem(x + k, 4)

    def local(src, dst, sem):
        copy = pltpu.make_async_copy(src, dst, sem)
        copy.start()
        return copy

    barrier = pltpu.get_barrier_semaphore()
    peers = [(ring1[0], tp), (ring1[1], tp), (ring2[0], tp), (ring2[1], tp)]
    peers += [(sp, lax.rem(tp + k, 8)) for k in range(1, 8)]
    for peer in peers:
        pl.semaphore_signal(barrier, inc=1, device_id=peer, device_id_type=MESH)

    first = [
        local(source, src_v, loc.at[0]),
        local(kw_in.at[0], kw.at[0], loc.at[1]),
        local(vw_in.at[0], vw.at[0], loc.at[2]),
        local(sgain, sg_v, loc.at[3]),
    ]
    target_load = [
        local(target.at[pl.ds(HALF * h, HALF)], xg.at[0, h, x], loc.at[(4, 9)[h]]) for h in (0, 1)
    ]
    def remote(src, dst, send, recv, device):
        pltpu.make_async_remote_copy(
            src_ref=src, dst_ref=dst, send_sem=send, recv_sem=recv,
            device_id=device, device_id_type=MESH,
        ).start()

    def await_bytes(ref, sem):
        pltpu.make_async_copy(ref, ref, sem).wait()

    def slot_of(fp, spos):
        return fp * 8 + spos

    for copy in first:
        copy.wait()
    second = [local(kw_in.at[1], kw.at[1], loc.at[7]), local(vw_in.at[1], vw.at[1], loc.at[8])]
    gains_load = local(tgains, tg_v, loc.at[5])
    q_load = local(qw_in, qw.at[c], loc.at[6])
    ff = dw_in.shape[1]
    late = [
        local(gw_in, raw.at[:, pl.ds(0, ff)], wts.at[0]),
        local(uw_in, raw.at[:, pl.ds(ff, ff)], wts.at[1]),
        local(dw_in, dn.at[c], wts.at[2]),
    ]
    own_rows = pl.ds(pl.multiple_of((c * 4 + x) * HD, HD), HD)
    own_out = [
        local(ow_in.at[l], ow.at[l, own_rows], own_sem.at[l]) for l in range(LAYERS)
    ]

    wide = src_v[...].astype(F32)
    scaled = wide * lax.rsqrt(jnp.mean(wide * wide, axis=-1, keepdims=True) + EPS)
    source_gains = sg_v[...].astype(F32)

    def project_source(l):
        normed = (scaled * source_gains[l : l + 1]).astype(BF)
        kv[l, slot_of(f, s), 0] = dot(normed, kw[l]).astype(BF)
        kv[l, slot_of(f, s), 1] = jnp.transpose(dot(normed, vw[l])).astype(BF)

    def send1(l, hop, way):
        delta = hop - 1
        fp = wrap(f - delta) if way == 0 else wrap(f + delta)
        block = kv.at[l, slot_of(fp, s)]
        if hop == 4:
            block = block.at[way]
        remote(block, block, kvs.at[l], r1.at[l, hop - 1, way], (ring1[way], tp))

    def recv1(l, hop, way):
        fp = wrap(f - hop) if way == 0 else wrap(f + hop)
        block = kv.at[l, slot_of(fp, s)]
        if hop == 4:
            block = block.at[way]
        await_bytes(block, r1.at[l, hop - 1, way])

    def send2(n, hop, way):
        l, k = divmod(n, 8)
        fp = wrap(f + ring_offset(k))
        delta = hop - 1
        spos = wrap(s - delta) if way == 0 else wrap(s + delta)
        block = kv.at[l, slot_of(fp, spos)]
        if hop == 4:
            block = block.at[way]
        remote(block, block, kvs.at[l], r2.at[n, hop - 1, way], (ring2[way], tp))

    def recv2(n, hop, way):
        l, k = divmod(n, 8)
        fp = wrap(f + ring_offset(k))
        spos = wrap(s - hop) if way == 0 else wrap(s + hop)
        block = kv.at[l, slot_of(fp, spos)]
        if hop == 4:
            block = block.at[way]
        await_bytes(block, r2.at[n, hop - 1, way])

    halves = {}
    waiting = []

    here, released = set(), set()

    def fresh(n):
        if n < 8 or (n in here and n in released):
            for w in (0, 1):
                send2(n, 1, w)

    def arrived(n):
        here.add(n)
        waiting.append((n // 8, n % 8, 0))
        fresh(n)

    def handle(event):
        ring, index, hop, way = event
        if ring == 3:
            released.add(index)
            fresh(index)
            return
        if ring == 0:
            for w in (0, 1):
                send1(index, 1, w)
            arrived(8 * index)
            return
        if hop == 4:
            halves[ring, index] = halves.get((ring, index), 0) + 1
        whole = hop < 4 or halves[ring, index] == 2
        if ring == 1:
            recv1(index, hop, way)
            if hop < 4:
                send1(index, hop + 1, way)
            if whole:
                arrived(8 * index + (2 * hop - way if hop < 4 else 7))
        else:
            recv2(index, hop, way)
            if hop < 4:
                send2(index, hop + 1, way)
            if whole:
                waiting.append((index // 8, index % 8, -hop if way == 0 else hop))

    groups = {0: [], 1: []}

    def attend(l, slots):
        done = groups[l]
        if slots is not None:
            keys = jnp.concatenate([kv[l, slot, 0] for slot in slots], axis=0)
            scores_ref[len(done) % 2] = dot(keys, qcat(l))
            done.append(slots)
        if len(done) == 1 and slots is not None:
            return
        past = -2 if slots is not None else -1
        values = jnp.concatenate([kv[l, slot, 1] for slot in done[past]], axis=1)
        scores = scores_ref[(len(done) + past) % 2]
        old = m_ref[...]
        new = jnp.maximum(old, jnp.max(scores, axis=0, keepdims=True))
        shrink = jnp.exp2(old - new)
        weights = jnp.exp2(scores - new)
        m_ref[...] = new
        l_ref[...] = l_ref[...] * shrink + jnp.sum(weights, axis=0, keepdims=True)
        acc_ref[...] = acc_ref[...] * shrink + dot(values, weights.astype(BF))

    def attend_waiting(l):
        blocks = [v for v in waiting if v[0] == l][:8]
        for v in blocks:
            waiting.remove(v)
        attend(l, [slot_of(wrap(f + ring_offset(k)), wrap(s + d)) for _, k, d in blocks])

    def qcat(l):
        return jnp.concatenate([qown[l], qrecv[l]], axis=1)

    def start_queries(l):
        gain = tg_v[l].astype(F32)[0:1]
        rows = xg[l].reshape(GROUP, D).astype(F32)
        normed = rms(rows, gain).astype(BF)
        theirs = dot(normed, qw[1 - c, l]) * QSCALE
        qsend[l] = jnp.transpose(theirs).astype(BF)
        remote(qsend.at[l], qrecv.at[l], q_send.at[l], q_recv.at[l], (sp, partner))
        mine = dot(normed, qw[c, l]) * QSCALE
        qown[l] = jnp.transpose(mine).astype(BF)
        m_ref[...] = jnp.full_like(m_ref, -1e30)
        l_ref[...] = jnp.zeros_like(l_ref)
        acc_ref[...] = jnp.zeros_like(acc_ref)

    def await_queries(l):
        await_bytes(qrecv.at[l], q_recv.at[l])

    def send_context(l):
        context = jnp.transpose(acc_ref[...] / l_ref[...]).astype(BF)
        slot = c * 4 + x
        csend[l] = context
        for h in (0, 1):
            mine = csend.at[l, pl.ds(h * PART, PART)]
            theirs = csend.at[l, pl.ds(GROUP + h * PART, PART)]
            here = cx.at[l, h, slot]
            for k in (2, 1, 3):
                chip = other_x(k) * 2
                remote(mine, here, c_send.at[l], c_recv.at[l, h], (sp, chip + c))
                remote(theirs, here, c_send.at[l], c_recv.at[l, h], (sp, chip + 1 - c))
            remote(theirs, here, c_send.at[l], c_recv.at[l, h], (sp, partner))
            cx[l, h, slot] = context[h * PART : (h + 1) * PART]

    def after_context(l, h):
        await_bytes(cx.at[l, h, pl.ds(0, 7)], c_recv.at[l, h])
        gains = tg_v[l].astype(F32)
        contexts = jnp.concatenate([cx[l, h, j] for j in range(8)], axis=1)
        attended = dot(contexts, ow[l]).astype(BF).astype(F32)
        rows = xg[l, h].reshape(PART, D).astype(F32)
        stream = (rows + rms(attended, gains[1:2])).astype(BF)
        mid[l, h] = stream.reshape(4, HALF, D)
        mixer_in = rms(stream.astype(F32), gains[2:3]).astype(BF)
        mixed = None
        for j in range(2):
            both = dot(mixer_in, gu[j, l])
            gate, up = both[:, :ff], both[:, ff:]
            hidden = (gate / (1.0 + jnp.exp(-gate)) * up).astype(BF)
            term = dot(hidden, dn[j, l])
            mixed = term if mixed is None else mixed + term
        rsend[l, h] = mixed.astype(BF).reshape(4, HALF, D)
        for k in (2, 1, 3):
            remote(
                rsend.at[l, h, other_x(k)], rs.at[l, h, x], s_send.at[l], s_recv.at[l, h],
                (sp, other_x(k) * 2 + c),
            )
        rs[l, h, x] = rsend[l, h, x]

    def after_sum(l, h):
        await_bytes(rs.at[l, h, pl.ds(0, 3)], s_recv.at[l, h])
        gain = tg_v[l].astype(F32)[3:4]
        total = rs[l, h, 0].astype(F32)
        for j in range(1, 4):
            total = total + rs[l, h, j].astype(F32)
        mixer_out = total.astype(BF).astype(F32)
        return mid[l, h, x].astype(F32) + rms(mixer_out, gain)

    def forward_out(l):
        own_out[l].wait()
        await_bytes(ow.at[l, pl.ds(0, 3 * HD)], o_recv.at[l])
        plane = pl.ds(pl.multiple_of(c * 512, 512), 512)
        remote(ow.at[l, plane], ow.at[l, plane], of_send.at[l], of_recv.at[l], (sp, partner))

    def send_target():
        for copy in target_load:
            copy.wait()
        for k in (2, 1, 3):
            remote(xg.at[0, :, x], xg.at[0, :, x], x_send.at[0], x_recv.at[0], (sp, other_x(k) * 2 + c))
        remote(qw_in, qw.at[c], pw_send.at[0], pw_recv.at[0], (sp, partner))

    def send_out(l):
        for k in (2, 1, 3):
            remote(
                ow_in.at[l], ow.at[l, own_rows], o_send.at[l], o_recv.at[l],
                (sp, other_x(k) * 2 + c),
            )

    def turn_ff():
        for copy in late:
            copy.wait()
        for l in range(LAYERS):
            gu[c, l] = jnp.transpose(raw[l])

    def send_ff():
        remote(gu.at[c], gu.at[c], pw_send.at[1], pw_recv.at[1], (sp, partner))
        remote(dw_in, dn.at[c], pw_send.at[2], pw_recv.at[2], (sp, partner))

    project_source(0)
    pl.semaphore_wait(barrier, len(peers))

    events = ring_events(LATENCY, SECOND_START, RELEASES)
    last_first = max(t for t, (r, i, _, _) in events if r in (1, 2) and i < (8 if r == 2 else 1))
    hooks = {}

    def run_until(limit, attending):
        while events and events[0][0] <= limit:
            when, event = events.pop(0)
            for hook_time in sorted(hooks):
                if hook_time <= when:
                    hooks.pop(hook_time)()
            handle(event)
            if attending is not None and sum(v[0] == attending for v in waiting) >= 8:
                attend_waiting(attending)

    hooks[20.0] = lambda: forward_out(0)
    hooks[29.0] = lambda: forward_out(1)
    run_until(0.0, None)
    send_target()
    for copy in second:
        copy.wait()
    project_source(1)
    send_out(0)
    turn_ff()
    run_until(6.0, None)
    send_out(1)
    gains_load.wait()
    q_load.wait()
    await_bytes(qw.at[0], pw_recv.at[0])
    await_bytes(xg.at[0, :, pl.ds(0, 3)], x_recv.at[0])
    start_queries(0)
    run_until(9.0, None)
    send_ff()
    await_queries(0)
    run_until(last_first, 0)
    attend(0, None)
    send_context(0)
    await_bytes(gu.at[0], pw_recv.at[1])
    await_bytes(dn.at[0], pw_recv.at[2])
    await_bytes(ow.at[0, pl.ds(0, 512)], of_recv.at[0])
    run_until(last_first + MARKS[0], None)
    after_context(0, 0)
    run_until(last_first + MARKS[1], None)
    after_context(0, 1)
    run_until(last_first + MARKS[2], None)
    for h in (0, 1):
        xg[1, h, x] = after_sum(0, h).astype(BF)
        for k in (2, 1, 3):
            remote(
                xg.at[1, h, x], xg.at[1, h, x], x_send.at[1], x_recv.at[1],
                (sp, other_x(k) * 2 + c),
            )
    run_until(last_first + MARKS[3], None)
    await_bytes(xg.at[1, :, pl.ds(0, 3)], x_recv.at[1])
    start_queries(1)
    run_until(last_first + MARKS[4], None)
    await_queries(1)
    while sum(v[0] == 1 for v in waiting) >= 8:
        attend_waiting(1)
    run_until(1000.0, 1)
    attend(1, None)
    send_context(1)
    await_bytes(ow.at[1, pl.ds(0, 512)], of_recv.at[1])
    after_context(1, 0)
    after_context(1, 1)
    for h in (0, 1):
        out[pl.ds(h * HALF, HALF)] = after_sum(1, h)

    for l in range(LAYERS):
        await_bytes(kv.at[l, pl.ds(0, 63)], kvs.at[l])
        await_bytes(xg.at[l, :, pl.ds(0, 3)], x_send.at[l])
        await_bytes(qsend.at[l], q_send.at[l])
        await_bytes(cx.at[l, :, pl.ds(0, 7)], c_send.at[l])
        await_bytes(rs.at[l, :, pl.ds(0, 3)], s_send.at[l])
        await_bytes(ow.at[l, pl.ds(0, 3 * HD)], o_send.at[l])
        await_bytes(ow.at[l, pl.ds(0, 512)], of_send.at[l])
    await_bytes(qw.at[0], pw_send.at[0])
    await_bytes(gu.at[0], pw_send.at[1])
    await_bytes(dn.at[0], pw_send.at[2])


def per_device(*args):
    args = list(args)
    ff = args[8].shape[2]
    args[8] = jnp.swapaxes(args[8], 1, 2)
    args[9] = jnp.swapaxes(args[9], 1, 2)
    hbm = pl.BlockSpec(memory_space=pl.ANY)
    vmem = pltpu.VMEM
    dma = pltpu.SemaphoreType.DMA
    scratch = [
        vmem((128, D), BF),
        vmem((LAYERS, 4, D), BF),
        vmem((LAYERS, D), BF),
        vmem((LAYERS, D, HD), BF),
        vmem((LAYERS, D, HD), BF),
        vmem((2, LAYERS, D, HD), BF),
        vmem((LAYERS, 2 * ff, D), BF),
        vmem((2, LAYERS, D, 2 * ff), BF),
        vmem((2, LAYERS, ff, D), BF),
        vmem((LAYERS, D, D), BF),
        vmem((LAYERS, BLOCKS, 2, HD, HD), BF),
        vmem((LAYERS, 2, 4, HALF, D), BF),
        vmem((LAYERS, HD, GROUP), BF),
        vmem((LAYERS, HD, GROUP), BF),
        vmem((LAYERS, HD, GROUP), BF),
        vmem((LAYERS, 2, 8, PART, HD), BF),
        vmem((LAYERS, 2 * GROUP, HD), BF),
        vmem((LAYERS, 2, 4, HALF, D), BF),
        vmem((LAYERS, 2, 4, HALF, D), BF),
        vmem((LAYERS, 2, 4, HALF, D), BF),
        vmem((1, 2 * GROUP), F32),
        vmem((1, 2 * GROUP), F32),
        vmem((HD, 2 * GROUP), F32),
        vmem((2, 8 * HD, 2 * GROUP), F32),
        dma((STEPS, 4, 2)),
        dma((LAYERS, 4, 2)),
        dma((LAYERS,)),
        dma((10,)),
        dma((3,)),
        dma((LAYERS,)),
    ]
    scratch += [dma((LAYERS,) + more) for more in ((), (), (), (), (2,), (), (2,), ())]
    scratch += [dma((3,)), dma((3,))]
    scratch += [dma((LAYERS,)) for _ in range(4)]
    wide = pl.pallas_call(
        kernel,
        out_shape=pltpu.VMEM((ROWS, D), F32),
        in_specs=[hbm] * 11,
        out_specs=pl.BlockSpec(memory_space=pltpu.VMEM),
        scratch_shapes=scratch,
        compiler_params=pltpu.CompilerParams(
            collective_id=0, has_side_effects=True, vmem_limit_bytes=60 * 1024 * 1024
        ),
    )(*args)
    return wide.astype(BF)


def solution(mesh):
    placed = (
        P(("sp", "tp"), None),
        P("sp", None),
        P(),
        P(),
        P(None, None, "tp"),
        P(None, None, "tp"),
        P(None, None, "tp"),
        P(None, "tp", None),
        P(None, None, "tp"),
        P(None, None, "tp"),
        P(None, "tp", None),
    )
    return jax.shard_map(
        per_device, mesh=mesh, in_specs=placed, out_specs=P(("sp", "tp"), None), check_vma=False
    )
```

```python
import functools
import math

import jax
import jax.numpy as jnp
from jax import lax
from jax.experimental import pallas as pl
from jax.experimental.pallas import tpu as pltpu
from jax.sharding import PartitionSpec as P

MESH = pl.DeviceIdType.MESH
BF = jnp.bfloat16
F32 = jnp.float32
EPS = 1e-06
HD = 128
D = 1024
ROWS = 32
GROUP = 128
HALF = ROWS // 2
PART = GROUP // 2
BLOCKS = 64
LAYERS = 2
STEPS = 8 * LAYERS
LATENCY = 2.5
EXCHANGE = 4.2
SWAP = 1.4
RELEASES = (26.2, 26.2, 30.3, 29.6, 31.5, 28.7, 29.2, 30.3)
QSCALE = HD ** (-0.5) * math.log2(math.e)


def rms(v, gain):
    inverse = lax.rsqrt(jnp.mean(v * v, axis=-1, keepdims=True) + EPS)
    return v * inverse * gain


def dot(a, b):
    return jnp.dot(a, b, preferred_element_type=F32)


def ring_offset(k):
    return ((k + 1) // 2) * (2 * (k % 2) - 1)


def plan(latency, exchange, swap, releases, block=0.7, cost=0.03):
    queues = {(way, ring): [] for way in (0, 1) for ring in (1, 2)}
    coming = [(0.0, (0, 0, 0, 0)), (1.0, (0, 1, 0, 0)), (6.0, (4, 0, 0, 0))]
    coming += [(t, (3, 8 + j, 0, 0)) for j, t in enumerate(releases)]
    ready, order = [], []
    here, released = set(), set()
    halves = {}
    blocks, taken, asked = [0, 0], [0, 0], [False, False]
    now = 0.0

    def put(ring, index, hop, way):
        queues[way, ring].append([block if hop < 4 else block / 2, (ring, index, hop, way)])

    def fresh(n):
        if n < 8 or (n in here and n in released):
            put(2, n, 1, 0)
            put(2, n, 1, 1)

    def arrived(n):
        here.add(n)
        blocks[n // 8] += 1
        fresh(n)

    def ends():
        for way in (0, 1):
            busy = [r for r in (1, 2) if queues[way, r]]
            for r in busy:
                yield queues[way, r][0], len(busy)

    def advance(span):
        nonlocal now
        end = now + span
        while now < end - 1e-9:
            step = min([end - now] + [item[0] * share for item, share in ends()])
            for item, share in list(ends()):
                item[0] -= step / share
            now += step
            for key in sorted(queues):
                if queues[key] and queues[key][0][0] < 1e-9:
                    coming.append((now + latency, queues[key].pop(0)[1]))

    while True:
        for v in [v for v in coming if v[0] <= now + 1e-9]:
            coming.remove(v)
            ready.append((0 if v[1][0] < 4 else 1, v[1]))
        for l in (0, 1):
            if asked[l] and blocks[l] - 8 * taken[l] >= 8 and (2, (8, l, 0, 0)) not in ready:
                ready.append((2, (8, l, 0, 0)))
        if not ready:
            times = [v[0] for v in coming] + [now + item[0] * share for item, share in ends()]
            advance(max(min(times) - now, 1e-6))
            continue
        ready.sort(key=lambda v: v[0])
        task = ready.pop(0)[1]
        order.append((now, task))
        kind, index, hop, way = task
        if kind == 0:
            put(1, index, 1, 0)
            put(1, index, 1, 1)
            arrived(8 * index)
        elif kind == 3:
            released.add(index)
            fresh(index)
        elif kind in (1, 2):
            if hop < 4:
                put(kind, index, hop + 1, way)
            else:
                halves[kind, index] = halves.get((kind, index), 0) + 1
            whole = hop < 4 or halves[kind, index] == 2
            if whole and kind == 1:
                arrived(8 * index + (2 * hop - way if hop < 4 else 7))
            elif whole:
                blocks[index // 8] += 1
        elif kind == 4:
            advance(0.7)
            coming.append((now + swap, (5, index, 0, 0)))
        elif kind == 5:
            asked[index] = True
        elif kind == 6:
            advance(1.35)
            coming.append((now + exchange - 0.6, (7, 0, hop, 0)))
        elif kind == 7:
            advance(0.1)
            if hop == 1:
                coming.append((now + exchange - 0.3, (4, 1, 0, 0)))
        elif kind == 8:
            taken[index] += 1
            advance(0.45)
            if taken[index] == 8:
                order.append((now, (9, index, 0, 0)))
                advance(0.45)
                if index == 1:
                    return order
                coming.append((now + exchange - 0.6, (6, 0, 0, 0)))
                coming.append((now + exchange + 0.8, (6, 0, 1, 0)))
        advance(cost)


def kernel(
    target, source, tgains, sgain, qw_in, kw_in, vw_in, ow_in, gw_in, uw_in, dw_in,
    out,
    src_v, tg_v, sg_v, kw, vw, qw, raw, gu, dn, ow,
    kv, xg, qown, qrecv, qsend, cx, csend, mid, rsend, rs,
    m_ref, l_ref, acc_ref, scores_ref,
    r2, r1, kvs, loc, wts, own_sem, x_recv, x_send, q_recv, q_send, c_recv, c_send, s_recv, s_send,
    pw_recv, pw_send, o_recv, o_send, of_recv, of_send,
):
    sp = lax.axis_index("sp")
    tp = lax.axis_index("tp")
    c = lax.rem(tp, 2)
    x = tp // 2
    z_pos, y_pos = sp // 8, lax.rem(sp, 8)
    f = (1 - c) * y_pos + c * z_pos
    s = (1 - c) * z_pos + c * y_pos

    def sp_of(fp, spos):
        return fp * (1 + 7 * c) + spos * (8 - 7 * c)

    def wrap(v):
        return lax.rem(v + 16, 8)

    ring1 = (sp_of(wrap(f + 1), s), sp_of(wrap(f - 1), s))
    ring2 = (sp_of(f, wrap(s + 1)), sp_of(f, wrap(s - 1)))
    partner = x * 2 + (1 - c)

    def other_x(k):
        return lax.rem(x + k, 4)

    def local(src, dst, sem):
        copy = pltpu.make_async_copy(src, dst, sem)
        copy.start()
        return copy

    barrier = pltpu.get_barrier_semaphore()
    peers = [(ring1[0], tp), (ring1[1], tp), (ring2[0], tp), (ring2[1], tp)]
    peers += [(sp, lax.rem(tp + k, 8)) for k in range(1, 8)]
    for peer in peers:
        pl.semaphore_signal(barrier, inc=1, device_id=peer, device_id_type=MESH)

    first = [
        local(source, src_v, loc.at[0]),
        local(kw_in.at[0], kw.at[0], loc.at[1]),
        local(vw_in.at[0], vw.at[0], loc.at[2]),
        local(sgain, sg_v, loc.at[3]),
    ]
    target_load = [
        local(target.at[pl.ds(HALF * h, HALF)], xg.at[0, h, x], loc.at[(4, 9)[h]]) for h in (0, 1)
    ]
    def remote(src, dst, send, recv, device):
        pltpu.make_async_remote_copy(
            src_ref=src, dst_ref=dst, send_sem=send, recv_sem=recv,
            device_id=device, device_id_type=MESH,
        ).start()

    def await_bytes(ref, sem):
        pltpu.make_async_copy(ref, ref, sem).wait()

    def slot_of(fp, spos):
        return fp * 8 + spos

    for copy in first:
        copy.wait()
    second = [local(kw_in.at[1], kw.at[1], loc.at[7]), local(vw_in.at[1], vw.at[1], loc.at[8])]
    gains_load = local(tgains, tg_v, loc.at[5])
    q_load = local(qw_in, qw.at[c], loc.at[6])
    ff = dw_in.shape[1]
    late = [
        local(gw_in, raw.at[:, pl.ds(0, ff)], wts.at[0]),
        local(uw_in, raw.at[:, pl.ds(ff, ff)], wts.at[1]),
        local(dw_in, dn.at[c], wts.at[2]),
    ]
    own_rows = pl.ds(pl.multiple_of((c * 4 + x) * HD, HD), HD)
    own_out = [
        local(ow_in.at[l], ow.at[l, own_rows], own_sem.at[l]) for l in range(LAYERS)
    ]

    wide = src_v[...].astype(F32)
    scaled = wide * lax.rsqrt(jnp.mean(wide * wide, axis=-1, keepdims=True) + EPS)
    source_gains = sg_v[...].astype(F32)

    def project_source(l):
        normed = (scaled * source_gains[l : l + 1]).astype(BF)
        kv[l, slot_of(f, s), 0] = dot(normed, kw[l]).astype(BF)
        kv[l, slot_of(f, s), 1] = jnp.transpose(dot(normed, vw[l])).astype(BF)

    def send1(l, hop, way):
        delta = hop - 1
        fp = wrap(f - delta) if way == 0 else wrap(f + delta)
        block = kv.at[l, slot_of(fp, s)]
        if hop == 4:
            block = block.at[way]
        remote(block, block, kvs.at[l], r1.at[l, hop - 1, way], (ring1[way], tp))

    def recv1(l, hop, way):
        fp = wrap(f - hop) if way == 0 else wrap(f + hop)
        block = kv.at[l, slot_of(fp, s)]
        if hop == 4:
            block = block.at[way]
        await_bytes(block, r1.at[l, hop - 1, way])

    def send2(n, hop, way):
        l, k = divmod(n, 8)
        fp = wrap(f + ring_offset(k))
        delta = hop - 1
        spos = wrap(s - delta) if way == 0 else wrap(s + delta)
        block = kv.at[l, slot_of(fp, spos)]
        if hop == 4:
            block = block.at[way]
        remote(block, block, kvs.at[l], r2.at[n, hop - 1, way], (ring2[way], tp))

    def recv2(n, hop, way):
        l, k = divmod(n, 8)
        fp = wrap(f + ring_offset(k))
        spos = wrap(s - hop) if way == 0 else wrap(s + hop)
        block = kv.at[l, slot_of(fp, spos)]
        if hop == 4:
            block = block.at[way]
        await_bytes(block, r2.at[n, hop - 1, way])

    halves = {}
    waiting = []

    here, released = set(), set()

    def fresh(n):
        if n < 8 or (n in here and n in released):
            for w in (0, 1):
                send2(n, 1, w)

    def arrived(n):
        here.add(n)
        waiting.append((n // 8, n % 8, 0))
        fresh(n)

    def handle(event):
        ring, index, hop, way = event
        if ring == 3:
            released.add(index)
            fresh(index)
            return
        if ring == 0:
            for w in (0, 1):
                send1(index, 1, w)
            arrived(8 * index)
            return
        if hop == 4:
            halves[ring, index] = halves.get((ring, index), 0) + 1
        whole = hop < 4 or halves[ring, index] == 2
        if ring == 1:
            recv1(index, hop, way)
            if hop < 4:
                send1(index, hop + 1, way)
            if whole:
                arrived(8 * index + (2 * hop - way if hop < 4 else 7))
        else:
            recv2(index, hop, way)
            if hop < 4:
                send2(index, hop + 1, way)
            if whole:
                waiting.append((index // 8, index % 8, -hop if way == 0 else hop))

    groups = {0: [], 1: []}

    def attend(l, slots):
        done = groups[l]
        if slots is not None:
            keys = jnp.concatenate([kv[l, slot, 0] for slot in slots], axis=0)
            scores_ref[len(done) % 2] = dot(keys, qcat(l))
            done.append(slots)
        if len(done) == 1 and slots is not None:
            return
        past = -2 if slots is not None else -1
        values = jnp.concatenate([kv[l, slot, 1] for slot in done[past]], axis=1)
        scores = scores_ref[(len(done) + past) % 2]
        old = m_ref[...]
        new = jnp.maximum(old, jnp.max(scores, axis=0, keepdims=True))
        shrink = jnp.exp2(old - new)
        weights = jnp.exp2(scores - new)
        m_ref[...] = new
        l_ref[...] = l_ref[...] * shrink + jnp.sum(weights, axis=0, keepdims=True)
        acc_ref[...] = acc_ref[...] * shrink + dot(values, weights.astype(BF))

    def attend_waiting(l):
        blocks = [v for v in waiting if v[0] == l][:8]
        for v in blocks:
            waiting.remove(v)
        attend(l, [slot_of(wrap(f + ring_offset(k)), wrap(s + d)) for _, k, d in blocks])

    def qcat(l):
        return jnp.concatenate([qown[l], qrecv[l]], axis=1)

    def start_queries(l):
        gain = tg_v[l].astype(F32)[0:1]
        rows = xg[l].reshape(GROUP, D).astype(F32)
        normed = rms(rows, gain).astype(BF)
        theirs = dot(normed, qw[1 - c, l]) * QSCALE
        qsend[l] = jnp.transpose(theirs).astype(BF)
        remote(qsend.at[l], qrecv.at[l], q_send.at[l], q_recv.at[l], (sp, partner))
        mine = dot(normed, qw[c, l]) * QSCALE
        qown[l] = jnp.transpose(mine).astype(BF)
        m_ref[...] = jnp.full_like(m_ref, -1e30)
        l_ref[...] = jnp.zeros_like(l_ref)
        acc_ref[...] = jnp.zeros_like(acc_ref)

    def await_queries(l):
        await_bytes(qrecv.at[l], q_recv.at[l])

    def send_context(l):
        context = jnp.transpose(acc_ref[...] / l_ref[...]).astype(BF)
        slot = c * 4 + x
        csend[l] = context
        for h in (0, 1):
            mine = csend.at[l, pl.ds(h * PART, PART)]
            theirs = csend.at[l, pl.ds(GROUP + h * PART, PART)]
            here = cx.at[l, h, slot]
            for k in (2, 1, 3):
                chip = other_x(k) * 2
                remote(mine, here, c_send.at[l], c_recv.at[l, h], (sp, chip + c))
                remote(theirs, here, c_send.at[l], c_recv.at[l, h], (sp, chip + 1 - c))
            remote(theirs, here, c_send.at[l], c_recv.at[l, h], (sp, partner))
            cx[l, h, slot] = context[h * PART : (h + 1) * PART]

    def after_context(l, h):
        await_bytes(cx.at[l, h, pl.ds(0, 7)], c_recv.at[l, h])
        gains = tg_v[l].astype(F32)
        contexts = jnp.concatenate([cx[l, h, j] for j in range(8)], axis=1)
        attended = dot(contexts, ow[l]).astype(BF).astype(F32)
        rows = xg[l, h].reshape(PART, D).astype(F32)
        stream = (rows + rms(attended, gains[1:2])).astype(BF)
        mid[l, h] = stream.reshape(4, HALF, D)
        mixer_in = rms(stream.astype(F32), gains[2:3]).astype(BF)
        mixed = None
        for j in range(2):
            both = dot(mixer_in, gu[j, l])
            gate, up = both[:, :ff], both[:, ff:]
            hidden = (gate / (1.0 + jnp.exp(-gate)) * up).astype(BF)
            term = dot(hidden, dn[j, l])
            mixed = term if mixed is None else mixed + term
        rsend[l, h] = mixed.astype(BF).reshape(4, HALF, D)
        for k in (2, 1, 3):
            remote(
                rsend.at[l, h, other_x(k)], rs.at[l, h, x], s_send.at[l], s_recv.at[l, h],
                (sp, other_x(k) * 2 + c),
            )
        rs[l, h, x] = rsend[l, h, x]

    def after_sum(l, h):
        await_bytes(rs.at[l, h, pl.ds(0, 3)], s_recv.at[l, h])
        gain = tg_v[l].astype(F32)[3:4]
        total = rs[l, h, 0].astype(F32)
        for j in range(1, 4):
            total = total + rs[l, h, j].astype(F32)
        mixer_out = total.astype(BF).astype(F32)
        return mid[l, h, x].astype(F32) + rms(mixer_out, gain)

    def forward_out(l):
        own_out[l].wait()
        await_bytes(ow.at[l, pl.ds(0, 3 * HD)], o_recv.at[l])
        plane = pl.ds(pl.multiple_of(c * 512, 512), 512)
        remote(ow.at[l, plane], ow.at[l, plane], of_send.at[l], of_recv.at[l], (sp, partner))

    def send_target():
        for copy in target_load:
            copy.wait()
        for k in (2, 1, 3):
            remote(xg.at[0, :, x], xg.at[0, :, x], x_send.at[0], x_recv.at[0], (sp, other_x(k) * 2 + c))
        remote(qw_in, qw.at[c], pw_send.at[0], pw_recv.at[0], (sp, partner))

    def send_out(l):
        for k in (2, 1, 3):
            remote(
                ow_in.at[l], ow.at[l, own_rows], o_send.at[l], o_recv.at[l],
                (sp, other_x(k) * 2 + c),
            )

    def turn_ff():
        for copy in late:
            copy.wait()
        for l in range(LAYERS):
            gu[c, l] = jnp.transpose(raw[l])

    def send_ff():
        remote(gu.at[c], gu.at[c], pw_send.at[1], pw_recv.at[1], (sp, partner))
        remote(dw_in, dn.at[c], pw_send.at[2], pw_recv.at[2], (sp, partner))

    project_source(0)
    pl.semaphore_wait(barrier, len(peers))

    def begin_queries(l):
        if l == 0:
            gains_load.wait()
            q_load.wait()
            await_bytes(qw.at[0], pw_recv.at[0])
        await_bytes(xg.at[l, :, pl.ds(0, 3)], x_recv.at[l])
        start_queries(l)
        if l == 0:
            send_out(1)
            send_ff()

    def end_attention(l):
        attend(l, None)
        send_context(l)
        if l == 0:
            await_bytes(gu.at[0], pw_recv.at[1])
            await_bytes(dn.at[0], pw_recv.at[2])
        await_bytes(ow.at[l, pl.ds(0, 512)], of_recv.at[l])

    def next_rows(h):
        xg[1, h, x] = after_sum(0, h).astype(BF)
        for k in (2, 1, 3):
            remote(
                xg.at[1, h, x], xg.at[1, h, x], x_send.at[1], x_recv.at[1],
                (sp, other_x(k) * 2 + c),
            )

    def after_start():
        send_target()
        for copy in second:
            copy.wait()
        project_source(1)
        send_out(0)
        turn_ff()

    hooks = [(0.01, after_start), (20.0, lambda: forward_out(0)), (29.0, lambda: forward_out(1))]
    for when, task in plan(LATENCY, EXCHANGE, SWAP, RELEASES):
        while hooks and hooks[0][0] <= when:
            hooks.pop(0)[1]()
        kind, index, hop, _ = task
        if kind < 4:
            handle(task)
        elif kind == 4:
            begin_queries(index)
        elif kind == 5:
            await_queries(index)
        elif kind == 6:
            after_context(index, hop)
        elif kind == 7:
            next_rows(hop)
        elif kind == 8:
            attend_waiting(index)
        else:
            end_attention(index)
    after_context(1, 0)
    after_context(1, 1)
    for h in (0, 1):
        out[pl.ds(h * HALF, HALF)] = after_sum(1, h)

    for l in range(LAYERS):
        await_bytes(kv.at[l, pl.ds(0, 63)], kvs.at[l])
        await_bytes(xg.at[l, :, pl.ds(0, 3)], x_send.at[l])
        await_bytes(qsend.at[l], q_send.at[l])
        await_bytes(cx.at[l, :, pl.ds(0, 7)], c_send.at[l])
        await_bytes(rs.at[l, :, pl.ds(0, 3)], s_send.at[l])
        await_bytes(ow.at[l, pl.ds(0, 3 * HD)], o_send.at[l])
        await_bytes(ow.at[l, pl.ds(0, 512)], of_send.at[l])
    await_bytes(qw.at[0], pw_send.at[0])
    await_bytes(gu.at[0], pw_send.at[1])
    await_bytes(dn.at[0], pw_send.at[2])


def per_device(*args):
    args = list(args)
    ff = args[8].shape[2]
    args[8] = jnp.swapaxes(args[8], 1, 2)
    args[9] = jnp.swapaxes(args[9], 1, 2)
    hbm = pl.BlockSpec(memory_space=pl.ANY)
    vmem = pltpu.VMEM
    dma = pltpu.SemaphoreType.DMA
    scratch = [
        vmem((128, D), BF),
        vmem((LAYERS, 4, D), BF),
        vmem((LAYERS, D), BF),
        vmem((LAYERS, D, HD), BF),
        vmem((LAYERS, D, HD), BF),
        vmem((2, LAYERS, D, HD), BF),
        vmem((LAYERS, 2 * ff, D), BF),
        vmem((2, LAYERS, D, 2 * ff), BF),
        vmem((2, LAYERS, ff, D), BF),
        vmem((LAYERS, D, D), BF),
        vmem((LAYERS, BLOCKS, 2, HD, HD), BF),
        vmem((LAYERS, 2, 4, HALF, D), BF),
        vmem((LAYERS, HD, GROUP), BF),
        vmem((LAYERS, HD, GROUP), BF),
        vmem((LAYERS, HD, GROUP), BF),
        vmem((LAYERS, 2, 8, PART, HD), BF),
        vmem((LAYERS, 2 * GROUP, HD), BF),
        vmem((LAYERS, 2, 4, HALF, D), BF),
        vmem((LAYERS, 2, 4, HALF, D), BF),
        vmem((LAYERS, 2, 4, HALF, D), BF),
        vmem((1, 2 * GROUP), F32),
        vmem((1, 2 * GROUP), F32),
        vmem((HD, 2 * GROUP), F32),
        vmem((2, 8 * HD, 2 * GROUP), F32),
        dma((STEPS, 4, 2)),
        dma((LAYERS, 4, 2)),
        dma((LAYERS,)),
        dma((10,)),
        dma((3,)),
        dma((LAYERS,)),
    ]
    scratch += [dma((LAYERS,) + more) for more in ((), (), (), (), (2,), (), (2,), ())]
    scratch += [dma((3,)), dma((3,))]
    scratch += [dma((LAYERS,)) for _ in range(4)]
    wide = pl.pallas_call(
        kernel,
        out_shape=pltpu.VMEM((ROWS, D), F32),
        in_specs=[hbm] * 11,
        out_specs=pl.BlockSpec(memory_space=pltpu.VMEM),
        scratch_shapes=scratch,
        compiler_params=pltpu.CompilerParams(
            collective_id=0, has_side_effects=True, vmem_limit_bytes=60 * 1024 * 1024
        ),
    )(*args)
    return wide.astype(BF)


def solution(mesh):
    placed = (
        P(("sp", "tp"), None),
        P("sp", None),
        P(),
        P(),
        P(None, None, "tp"),
        P(None, None, "tp"),
        P(None, None, "tp"),
        P(None, "tp", None),
        P(None, None, "tp"),
        P(None, None, "tp"),
        P(None, "tp", None),
    )
    return jax.shard_map(
        per_device, mesh=mesh, in_specs=placed, out_specs=P(("sp", "tp"), None), check_vma=False
    )
```

```python
import functools
import math

import jax
import jax.numpy as jnp
from jax import lax
from jax.experimental import pallas as pl
from jax.experimental.pallas import tpu as pltpu
from jax.sharding import PartitionSpec as P

MESH = pl.DeviceIdType.MESH
BF = jnp.bfloat16
F32 = jnp.float32
EPS = 1e-06
HD = 128
D = 1024
ROWS = 32
GROUP = 128
HALF = ROWS // 2
PART = GROUP // 2
BLOCKS = 64
LAYERS = 2
STEPS = 8 * LAYERS
LATENCY = 2.5
EXCHANGE = 4.2
SWAP = 1.4
RELEASES = (26.2, 26.2, 30.3, 29.6, 31.5, 28.7, 29.2, 30.3)
QSCALE = HD ** (-0.5) * math.log2(math.e)


def rms(v, gain):
    inverse = lax.rsqrt(jnp.mean(v * v, axis=-1, keepdims=True) + EPS)
    return v * inverse * gain


def dot(a, b):
    return jnp.dot(a, b, preferred_element_type=F32)


def ring_offset(k):
    return ((k + 1) // 2) * (2 * (k % 2) - 1)


def plan(latency, exchange, swap, releases, block=0.7, cost=0.03):
    queues = {(way, ring): [] for way in (0, 1) for ring in (1, 2)}
    coming = [(0.0, (0, 0, 0, 0)), (1.0, (0, 1, 0, 0)), (9.0, (4, 0, 0, 0))]
    coming += [(t, (3, 8 + j, 0, 0)) for j, t in enumerate(releases)]
    ready, order = [], []
    here, released = set(), set()
    halves = {}
    blocks, taken, asked = [0, 0], [0, 0], [False, False]
    now = 0.0

    def put(ring, index, hop, way):
        queues[way, ring].append([block if hop < 4 else block / 2, (ring, index, hop, way)])

    def fresh(n):
        if n < 8 or (n in here and n in released):
            put(2, n, 1, 0)
            put(2, n, 1, 1)

    def arrived(n):
        here.add(n)
        blocks[n // 8] += 1
        fresh(n)

    def ends():
        for way in (0, 1):
            busy = [r for r in (1, 2) if queues[way, r]]
            for r in busy:
                yield queues[way, r][0], len(busy)

    def advance(span):
        nonlocal now
        end = now + span
        while now < end - 1e-9:
            step = min([end - now] + [item[0] * share for item, share in ends()])
            for item, share in list(ends()):
                item[0] -= step / share
            now += step
            for key in sorted(queues):
                if queues[key] and queues[key][0][0] < 1e-9:
                    coming.append((now + latency, queues[key].pop(0)[1]))

    while True:
        for v in [v for v in coming if v[0] <= now + 1e-9]:
            coming.remove(v)
            ready.append((0 if v[1][0] < 4 else 1, v[1]))
        for l in (0, 1):
            if asked[l] and blocks[l] - 8 * taken[l] >= 8 and (2, (8, l, 0, 0)) not in ready:
                ready.append((2, (8, l, 0, 0)))
        if not ready:
            times = [v[0] for v in coming] + [now + item[0] * share for item, share in ends()]
            advance(max(min(times) - now, 1e-6))
            continue
        ready.sort(key=lambda v: v[0])
        task = ready.pop(0)[1]
        order.append((now, task))
        kind, index, hop, way = task
        if kind == 0:
            put(1, index, 1, 0)
            put(1, index, 1, 1)
            arrived(8 * index)
        elif kind == 3:
            released.add(index)
            fresh(index)
        elif kind in (1, 2):
            if hop < 4:
                put(kind, index, hop + 1, way)
            else:
                halves[kind, index] = halves.get((kind, index), 0) + 1
            whole = hop < 4 or halves[kind, index] == 2
            if whole and kind == 1:
                arrived(8 * index + (2 * hop - way if hop < 4 else 7))
            elif whole:
                blocks[index // 8] += 1
        elif kind == 4:
            advance(0.7)
            coming.append((now + (swap if index else 3.0), (5, index, 0, 0)))
        elif kind == 5:
            asked[index] = True
        elif kind == 6:
            advance(1.35)
            coming.append((now + exchange - 0.6, (7, 0, hop, 0)))
        elif kind == 7:
            advance(0.1)
            if hop == 1:
                coming.append((now + exchange - 0.3, (4, 1, 0, 0)))
        elif kind == 8:
            taken[index] += 1
            advance(0.45)
            if taken[index] == 8:
                order.append((now, (9, index, 0, 0)))
                advance(0.45)
                if index == 1:
                    return order
                coming.append((now + exchange - 0.6, (6, 0, 0, 0)))
                coming.append((now + exchange + 0.8, (6, 0, 1, 0)))
        advance(cost)


def kernel(
    target, source, tgains, sgain, qw_in, kw_in, vw_in, ow_in, gw_in, uw_in, dw_in,
    out,
    src_v, tg_v, sg_v, kw, vw, qw, raw, gu, dn, ow,
    kv, xg, qown, qrecv, qsend, cx, csend, mid, rsend, rs,
    m_ref, l_ref, acc_ref, scores_ref,
    r2, r1, kvs, loc, wts, own_sem, x_recv, x_send, q_recv, q_send, c_recv, c_send, s_recv, s_send,
    pw_recv, pw_send, o_recv, o_send, of_recv, of_send,
):
    sp = lax.axis_index("sp")
    tp = lax.axis_index("tp")
    c = lax.rem(tp, 2)
    x = tp // 2
    z_pos, y_pos = sp // 8, lax.rem(sp, 8)
    f = (1 - c) * y_pos + c * z_pos
    s = (1 - c) * z_pos + c * y_pos

    def sp_of(fp, spos):
        return fp * (1 + 7 * c) + spos * (8 - 7 * c)

    def wrap(v):
        return lax.rem(v + 16, 8)

    ring1 = (sp_of(wrap(f + 1), s), sp_of(wrap(f - 1), s))
    ring2 = (sp_of(f, wrap(s + 1)), sp_of(f, wrap(s - 1)))
    partner = x * 2 + (1 - c)

    def other_x(k):
        return lax.rem(x + k, 4)

    def local(src, dst, sem):
        copy = pltpu.make_async_copy(src, dst, sem)
        copy.start()
        return copy

    barrier = pltpu.get_barrier_semaphore()
    peers = [(ring1[0], tp), (ring1[1], tp), (ring2[0], tp), (ring2[1], tp)]
    peers += [(sp, lax.rem(tp + k, 8)) for k in range(1, 8)]
    for peer in peers:
        pl.semaphore_signal(barrier, inc=1, device_id=peer, device_id_type=MESH)

    first = [
        local(source, src_v, loc.at[0]),
        local(kw_in.at[0], kw.at[0], loc.at[1]),
        local(vw_in.at[0], vw.at[0], loc.at[2]),
        local(sgain, sg_v, loc.at[3]),
    ]
    target_load = [
        local(target.at[pl.ds(HALF * h, HALF)], xg.at[0, h, x], loc.at[(4, 9)[h]]) for h in (0, 1)
    ]
    def remote(src, dst, send, recv, device):
        pltpu.make_async_remote_copy(
            src_ref=src, dst_ref=dst, send_sem=send, recv_sem=recv,
            device_id=device, device_id_type=MESH,
        ).start()

    def await_bytes(ref, sem):
        pltpu.make_async_copy(ref, ref, sem).wait()

    def slot_of(fp, spos):
        return fp * 8 + spos

    for copy in first:
        copy.wait()
    second = [local(kw_in.at[1], kw.at[1], loc.at[7]), local(vw_in.at[1], vw.at[1], loc.at[8])]
    gains_load = local(tgains, tg_v, loc.at[5])
    q_load = local(qw_in, qw.at[c], loc.at[6])
    ff = dw_in.shape[1]
    late = [
        local(gw_in, raw.at[:, pl.ds(0, ff)], wts.at[0]),
        local(uw_in, raw.at[:, pl.ds(ff, ff)], wts.at[1]),
        local(dw_in, dn.at[c], wts.at[2]),
    ]
    own_rows = pl.ds(pl.multiple_of((c * 4 + x) * HD, HD), HD)
    own_out = [
        local(ow_in.at[l], ow.at[l, own_rows], own_sem.at[l]) for l in range(LAYERS)
    ]

    wide = src_v[...].astype(F32)
    scaled = wide * lax.rsqrt(jnp.mean(wide * wide, axis=-1, keepdims=True) + EPS)
    source_gains = sg_v[...].astype(F32)

    def project_source(l):
        normed = (scaled * source_gains[l : l + 1]).astype(BF)
        kv[l, slot_of(f, s), 0] = dot(normed, kw[l]).astype(BF)
        kv[l, slot_of(f, s), 1] = jnp.transpose(dot(normed, vw[l])).astype(BF)

    def send1(l, hop, way):
        delta = hop - 1
        fp = wrap(f - delta) if way == 0 else wrap(f + delta)
        block = kv.at[l, slot_of(fp, s)]
        if hop == 4:
            block = block.at[way]
        remote(block, block, kvs.at[l], r1.at[l, hop - 1, way], (ring1[way], tp))

    def recv1(l, hop, way):
        fp = wrap(f - hop) if way == 0 else wrap(f + hop)
        block = kv.at[l, slot_of(fp, s)]
        if hop == 4:
            block = block.at[way]
        await_bytes(block, r1.at[l, hop - 1, way])

    def send2(n, hop, way):
        l, k = divmod(n, 8)
        fp = wrap(f + ring_offset(k))
        delta = hop - 1
        spos = wrap(s - delta) if way == 0 else wrap(s + delta)
        block = kv.at[l, slot_of(fp, spos)]
        if hop == 4:
            block = block.at[way]
        remote(block, block, kvs.at[l], r2.at[n, hop - 1, way], (ring2[way], tp))

    def recv2(n, hop, way):
        l, k = divmod(n, 8)
        fp = wrap(f + ring_offset(k))
        spos = wrap(s - hop) if way == 0 else wrap(s + hop)
        block = kv.at[l, slot_of(fp, spos)]
        if hop == 4:
            block = block.at[way]
        await_bytes(block, r2.at[n, hop - 1, way])

    halves = {}
    waiting = []

    here, released = set(), set()

    def fresh(n):
        if n < 8 or (n in here and n in released):
            for w in (0, 1):
                send2(n, 1, w)

    def arrived(n):
        here.add(n)
        waiting.append((n // 8, n % 8, 0))
        fresh(n)

    def handle(event):
        ring, index, hop, way = event
        if ring == 3:
            released.add(index)
            fresh(index)
            return
        if ring == 0:
            for w in (0, 1):
                send1(index, 1, w)
            arrived(8 * index)
            return
        if hop == 4:
            halves[ring, index] = halves.get((ring, index), 0) + 1
        whole = hop < 4 or halves[ring, index] == 2
        if ring == 1:
            recv1(index, hop, way)
            if hop < 4:
                send1(index, hop + 1, way)
            if whole:
                arrived(8 * index + (2 * hop - way if hop < 4 else 7))
        else:
            recv2(index, hop, way)
            if hop < 4:
                send2(index, hop + 1, way)
            if whole:
                waiting.append((index // 8, index % 8, -hop if way == 0 else hop))

    groups = {0: [], 1: []}

    def attend(l, slots):
        done = groups[l]
        if slots is not None:
            keys = jnp.concatenate([kv[l, slot, 0] for slot in slots], axis=0)
            scores_ref[len(done) % 2] = dot(keys, qcat(l))
            done.append(slots)
        if len(done) == 1 and slots is not None:
            return
        past = -2 if slots is not None else -1
        values = jnp.concatenate([kv[l, slot, 1] for slot in done[past]], axis=1)
        scores = scores_ref[(len(done) + past) % 2]
        old = m_ref[...]
        new = jnp.maximum(old, jnp.max(scores, axis=0, keepdims=True))
        shrink = jnp.exp2(old - new)
        weights = jnp.exp2(scores - new)
        m_ref[...] = new
        l_ref[...] = l_ref[...] * shrink + jnp.sum(weights, axis=0, keepdims=True)
        acc_ref[...] = acc_ref[...] * shrink + dot(values, weights.astype(BF))

    def attend_waiting(l):
        blocks = [v for v in waiting if v[0] == l][:8]
        for v in blocks:
            waiting.remove(v)
        attend(l, [slot_of(wrap(f + ring_offset(k)), wrap(s + d)) for _, k, d in blocks])

    def qcat(l):
        return jnp.concatenate([qown[l], qrecv[l]], axis=1)

    def start_queries(l):
        gain = tg_v[l].astype(F32)[0:1]
        rows = xg[l].reshape(GROUP, D).astype(F32)
        normed = rms(rows, gain).astype(BF)
        theirs = dot(normed, qw[1 - c, l]) * QSCALE
        qsend[l] = jnp.transpose(theirs).astype(BF)
        remote(qsend.at[l], qrecv.at[l], q_send.at[l], q_recv.at[l], (sp, partner))
        mine = dot(normed, qw[c, l]) * QSCALE
        qown[l] = jnp.transpose(mine).astype(BF)
        m_ref[...] = jnp.full_like(m_ref, -1e30)
        l_ref[...] = jnp.zeros_like(l_ref)
        acc_ref[...] = jnp.zeros_like(acc_ref)

    def await_queries(l):
        await_bytes(qrecv.at[l], q_recv.at[l])

    def send_context(l):
        context = jnp.transpose(acc_ref[...] / l_ref[...]).astype(BF)
        slot = c * 4 + x
        csend[l] = context
        for h in (0, 1):
            mine = csend.at[l, pl.ds(h * PART, PART)]
            theirs = csend.at[l, pl.ds(GROUP + h * PART, PART)]
            here = cx.at[l, h, slot]
            for k in (2, 1, 3):
                chip = other_x(k) * 2
                remote(mine, here, c_send.at[l], c_recv.at[l, h], (sp, chip + c))
                remote(theirs, here, c_send.at[l], c_recv.at[l, h], (sp, chip + 1 - c))
            remote(theirs, here, c_send.at[l], c_recv.at[l, h], (sp, partner))
            cx[l, h, slot] = context[h * PART : (h + 1) * PART]

    def after_context(l, h):
        await_bytes(cx.at[l, h, pl.ds(0, 7)], c_recv.at[l, h])
        gains = tg_v[l].astype(F32)
        contexts = jnp.concatenate([cx[l, h, j] for j in range(8)], axis=1)
        attended = dot(contexts, ow[l]).astype(BF).astype(F32)
        rows = xg[l, h].reshape(PART, D).astype(F32)
        stream = (rows + rms(attended, gains[1:2])).astype(BF)
        mid[l, h] = stream.reshape(4, HALF, D)
        mixer_in = rms(stream.astype(F32), gains[2:3]).astype(BF)
        mixed = None
        for j in range(2):
            both = dot(mixer_in, gu[j, l])
            gate, up = both[:, :ff], both[:, ff:]
            hidden = (gate / (1.0 + jnp.exp(-gate)) * up).astype(BF)
            term = dot(hidden, dn[j, l])
            mixed = term if mixed is None else mixed + term
        rsend[l, h] = mixed.astype(BF).reshape(4, HALF, D)
        for k in (2, 1, 3):
            remote(
                rsend.at[l, h, other_x(k)], rs.at[l, h, x], s_send.at[l], s_recv.at[l, h],
                (sp, other_x(k) * 2 + c),
            )
        rs[l, h, x] = rsend[l, h, x]

    def after_sum(l, h):
        await_bytes(rs.at[l, h, pl.ds(0, 3)], s_recv.at[l, h])
        gain = tg_v[l].astype(F32)[3:4]
        total = rs[l, h, 0].astype(F32)
        for j in range(1, 4):
            total = total + rs[l, h, j].astype(F32)
        mixer_out = total.astype(BF).astype(F32)
        return mid[l, h, x].astype(F32) + rms(mixer_out, gain)

    def forward_out(l):
        own_out[l].wait()
        await_bytes(ow.at[l, pl.ds(0, 3 * HD)], o_recv.at[l])
        plane = pl.ds(pl.multiple_of(c * 512, 512), 512)
        remote(ow.at[l, plane], ow.at[l, plane], of_send.at[l], of_recv.at[l], (sp, partner))

    def send_target():
        for copy in target_load:
            copy.wait()
        for k in (2, 1, 3):
            remote(xg.at[0, :, x], xg.at[0, :, x], x_send.at[0], x_recv.at[0], (sp, other_x(k) * 2 + c))
        remote(qw_in, qw.at[c], pw_send.at[0], pw_recv.at[0], (sp, partner))

    def send_out(l):
        for k in (2, 1, 3):
            remote(
                ow_in.at[l], ow.at[l, own_rows], o_send.at[l], o_recv.at[l],
                (sp, other_x(k) * 2 + c),
            )

    def turn_ff():
        for copy in late:
            copy.wait()
        for l in range(LAYERS):
            gu[c, l] = jnp.transpose(raw[l])

    def send_ff():
        remote(gu.at[c], gu.at[c], pw_send.at[1], pw_recv.at[1], (sp, partner))
        remote(dw_in, dn.at[c], pw_send.at[2], pw_recv.at[2], (sp, partner))

    project_source(0)
    pl.semaphore_wait(barrier, len(peers))

    def begin_queries(l):
        if l == 0:
            gains_load.wait()
            q_load.wait()
            await_bytes(qw.at[0], pw_recv.at[0])
        await_bytes(xg.at[l, :, pl.ds(0, 3)], x_recv.at[l])
        start_queries(l)
        if l == 0:
            send_out(0)
            send_ff()

    def end_attention(l):
        attend(l, None)
        send_context(l)
        if l == 0:
            await_bytes(gu.at[0], pw_recv.at[1])
            await_bytes(dn.at[0], pw_recv.at[2])
        await_bytes(ow.at[l, pl.ds(0, 512)], of_recv.at[l])

    def next_rows(h):
        xg[1, h, x] = after_sum(0, h).astype(BF)
        for k in (2, 1, 3):
            remote(
                xg.at[1, h, x], xg.at[1, h, x], x_send.at[1], x_recv.at[1],
                (sp, other_x(k) * 2 + c),
            )

    def after_start():
        send_target()
        for copy in second:
            copy.wait()
        project_source(1)
        turn_ff()

    hooks = [(0.01, after_start), (15.0, lambda: send_out(1)), (23.0, lambda: forward_out(0)), (32.0, lambda: forward_out(1))]
    for when, task in plan(LATENCY, EXCHANGE, SWAP, RELEASES):
        while hooks and hooks[0][0] <= when:
            hooks.pop(0)[1]()
        kind, index, hop, _ = task
        if kind < 4:
            handle(task)
        elif kind == 4:
            begin_queries(index)
        elif kind == 5:
            await_queries(index)
        elif kind == 6:
            after_context(index, hop)
        elif kind == 7:
            next_rows(hop)
        elif kind == 8:
            attend_waiting(index)
        else:
            end_attention(index)
    after_context(1, 0)
    after_context(1, 1)
    for h in (0, 1):
        out[pl.ds(h * HALF, HALF)] = after_sum(1, h)

    for l in range(LAYERS):
        await_bytes(kv.at[l, pl.ds(0, 63)], kvs.at[l])
        await_bytes(xg.at[l, :, pl.ds(0, 3)], x_send.at[l])
        await_bytes(qsend.at[l], q_send.at[l])
        await_bytes(cx.at[l, :, pl.ds(0, 7)], c_send.at[l])
        await_bytes(rs.at[l, :, pl.ds(0, 3)], s_send.at[l])
        await_bytes(ow.at[l, pl.ds(0, 3 * HD)], o_send.at[l])
        await_bytes(ow.at[l, pl.ds(0, 512)], of_send.at[l])
    await_bytes(qw.at[0], pw_send.at[0])
    await_bytes(gu.at[0], pw_send.at[1])
    await_bytes(dn.at[0], pw_send.at[2])


def per_device(*args):
    args = list(args)
    ff = args[8].shape[2]
    args[8] = jnp.swapaxes(args[8], 1, 2)
    args[9] = jnp.swapaxes(args[9], 1, 2)
    hbm = pl.BlockSpec(memory_space=pl.ANY)
    vmem = pltpu.VMEM
    dma = pltpu.SemaphoreType.DMA
    scratch = [
        vmem((128, D), BF),
        vmem((LAYERS, 4, D), BF),
        vmem((LAYERS, D), BF),
        vmem((LAYERS, D, HD), BF),
        vmem((LAYERS, D, HD), BF),
        vmem((2, LAYERS, D, HD), BF),
        vmem((LAYERS, 2 * ff, D), BF),
        vmem((2, LAYERS, D, 2 * ff), BF),
        vmem((2, LAYERS, ff, D), BF),
        vmem((LAYERS, D, D), BF),
        vmem((LAYERS, BLOCKS, 2, HD, HD), BF),
        vmem((LAYERS, 2, 4, HALF, D), BF),
        vmem((LAYERS, HD, GROUP), BF),
        vmem((LAYERS, HD, GROUP), BF),
        vmem((LAYERS, HD, GROUP), BF),
        vmem((LAYERS, 2, 8, PART, HD), BF),
        vmem((LAYERS, 2 * GROUP, HD), BF),
        vmem((LAYERS, 2, 4, HALF, D), BF),
        vmem((LAYERS, 2, 4, HALF, D), BF),
        vmem((LAYERS, 2, 4, HALF, D), BF),
        vmem((1, 2 * GROUP), F32),
        vmem((1, 2 * GROUP), F32),
        vmem((HD, 2 * GROUP), F32),
        vmem((2, 8 * HD, 2 * GROUP), F32),
        dma((STEPS, 4, 2)),
        dma((LAYERS, 4, 2)),
        dma((LAYERS,)),
        dma((10,)),
        dma((3,)),
        dma((LAYERS,)),
    ]
    scratch += [dma((LAYERS,) + more) for more in ((), (), (), (), (2,), (), (2,), ())]
    scratch += [dma((3,)), dma((3,))]
    scratch += [dma((LAYERS,)) for _ in range(4)]
    wide = pl.pallas_call(
        kernel,
        out_shape=pltpu.VMEM((ROWS, D), F32),
        in_specs=[hbm] * 11,
        out_specs=pl.BlockSpec(memory_space=pltpu.VMEM),
        scratch_shapes=scratch,
        compiler_params=pltpu.CompilerParams(
            collective_id=0, has_side_effects=True, vmem_limit_bytes=60 * 1024 * 1024
        ),
    )(*args)
    return wide.astype(BF)


def solution(mesh):
    placed = (
        P(("sp", "tp"), None),
        P("sp", None),
        P(),
        P(),
        P(None, None, "tp"),
        P(None, None, "tp"),
        P(None, None, "tp"),
        P(None, "tp", None),
        P(None, None, "tp"),
        P(None, None, "tp"),
        P(None, "tp", None),
    )
    return jax.shard_map(
        per_device, mesh=mesh, in_specs=placed, out_specs=P(("sp", "tp"), None), check_vma=False
    )
```

```python
import functools
import math

import jax
import jax.numpy as jnp
from jax import lax
from jax.experimental import pallas as pl
from jax.experimental.pallas import tpu as pltpu
from jax.sharding import PartitionSpec as P

MESH = pl.DeviceIdType.MESH
BF = jnp.bfloat16
F32 = jnp.float32
EPS = 1e-06
HD = 128
D = 1024
ROWS = 32
GROUP = 128
HALF = ROWS // 2
PART = GROUP // 2
BLOCKS = 64
LAYERS = 2
STEPS = 8 * LAYERS
LATENCY = 2.5
EXCHANGE = 4.2
SWAP = 1.4
RELEASES = (26.2, 26.2, 30.3, 29.6, 31.5, 28.7, 29.2, 30.3)
QSCALE = HD ** (-0.5) * math.log2(math.e)


def rms(v, gain):
    inverse = lax.rsqrt(jnp.mean(v * v, axis=-1, keepdims=True) + EPS)
    return v * inverse * gain


def dot(a, b):
    return jnp.dot(a, b, preferred_element_type=F32)


def ring_offset(k):
    return ((k + 1) // 2) * (2 * (k % 2) - 1)


def plan(latency, exchange, swap, releases, block=0.7, cost=0.03):
    queues = {(way, ring): [] for way in (0, 1) for ring in (1, 2)}
    coming = [(0.0, (0, 0, 0, 0)), (1.0, (0, 1, 0, 0)), (8.2, (4, 0, 0, 0))]
    coming += [(t, (3, 8 + j, 0, 0)) for j, t in enumerate(releases)]
    ready, order = [], []
    here, released = set(), set()
    halves = {}
    blocks, taken, asked = [0, 0], [0, 0], [False, False]
    now = 0.0

    def put(ring, index, hop, way):
        queues[way, ring].append([block if hop < 4 else block / 2, (ring, index, hop, way)])

    def fresh(n):
        if n < 8 or (n in here and n in released):
            put(2, n, 1, 0)
            put(2, n, 1, 1)

    def arrived(n):
        here.add(n)
        blocks[n // 8] += 1
        fresh(n)

    def ends():
        for way in (0, 1):
            busy = [r for r in (1, 2) if queues[way, r]]
            for r in busy:
                yield queues[way, r][0], len(busy)

    def advance(span):
        nonlocal now
        end = now + span
        while now < end - 1e-9:
            step = min([end - now] + [item[0] * share for item, share in ends()])
            for item, share in list(ends()):
                item[0] -= step / share
            now += step
            for key in sorted(queues):
                if queues[key] and queues[key][0][0] < 1e-9:
                    coming.append((now + latency, queues[key].pop(0)[1]))

    while True:
        for v in [v for v in coming if v[0] <= now + 1e-9]:
            coming.remove(v)
            ready.append((0 if v[1][0] < 4 else 1, v[1]))
        for l in (0, 1):
            if asked[l] and blocks[l] - 8 * taken[l] >= 8 and (2, (8, l, 0, 0)) not in ready:
                ready.append((2, (8, l, 0, 0)))
        if not ready:
            times = [v[0] for v in coming] + [now + item[0] * share for item, share in ends()]
            advance(max(min(times) - now, 1e-6))
            continue
        ready.sort(key=lambda v: v[0])
        task = ready.pop(0)[1]
        order.append((now, task))
        kind, index, hop, way = task
        if kind == 0:
            put(1, index, 1, 0)
            put(1, index, 1, 1)
            arrived(8 * index)
        elif kind == 3:
            released.add(index)
            fresh(index)
        elif kind in (1, 2):
            if hop < 4:
                put(kind, index, hop + 1, way)
            else:
                halves[kind, index] = halves.get((kind, index), 0) + 1
            whole = hop < 4 or halves[kind, index] == 2
            if whole and kind == 1:
                arrived(8 * index + (2 * hop - way if hop < 4 else 7))
            elif whole:
                blocks[index // 8] += 1
        elif kind == 4:
            advance(0.7)
            coming.append((now + (swap if index else 3.0), (5, index, 0, 0)))
        elif kind == 5:
            asked[index] = True
        elif kind == 6:
            advance(1.35)
            coming.append((now + exchange - 0.6, (7, 0, hop, 0)))
        elif kind == 7:
            advance(0.1)
            if hop == 1:
                coming.append((now + exchange - 0.3, (4, 1, 0, 0)))
        elif kind == 8:
            taken[index] += 1
            advance(0.45)
            if taken[index] == 8:
                order.append((now, (9, index, 0, 0)))
                advance(0.45)
                if index == 1:
                    return order
                coming.append((now + exchange - 0.6, (6, 0, 0, 0)))
                coming.append((now + exchange + 0.8, (6, 0, 1, 0)))
        advance(cost)


def kernel(
    target, source, tgains, sgain, qw_in, kw_in, vw_in, ow_in, gw_in, uw_in, dw_in,
    out,
    src_v, tg_v, sg_v, kw, vw, qw, raw, gu, dn, ow,
    kv, xg, qown, qrecv, qsend, cx, csend, mid, rsend, rs,
    m_ref, l_ref, acc_ref, scores_ref,
    r2, r1, kvs, loc, wts, own_sem, x_recv, x_send, q_recv, q_send, c_recv, c_send, s_recv, s_send,
    pw_recv, pw_send, o_recv, o_send, of_recv, of_send,
):
    sp = lax.axis_index("sp")
    tp = lax.axis_index("tp")
    c = lax.rem(tp, 2)
    x = tp // 2
    z_pos, y_pos = sp // 8, lax.rem(sp, 8)
    f = (1 - c) * y_pos + c * z_pos
    s = (1 - c) * z_pos + c * y_pos

    def sp_of(fp, spos):
        return fp * (1 + 7 * c) + spos * (8 - 7 * c)

    def wrap(v):
        return lax.rem(v + 16, 8)

    ring1 = (sp_of(wrap(f + 1), s), sp_of(wrap(f - 1), s))
    ring2 = (sp_of(f, wrap(s + 1)), sp_of(f, wrap(s - 1)))
    partner = x * 2 + (1 - c)

    def other_x(k):
        return lax.rem(x + k, 4)

    def local(src, dst, sem):
        copy = pltpu.make_async_copy(src, dst, sem)
        copy.start()
        return copy

    barrier = pltpu.get_barrier_semaphore()
    peers = [(ring1[0], tp), (ring1[1], tp), (ring2[0], tp), (ring2[1], tp)]
    peers += [(sp, lax.rem(tp + k, 8)) for k in range(1, 8)]
    for peer in peers:
        pl.semaphore_signal(barrier, inc=1, device_id=peer, device_id_type=MESH)

    first = [
        local(source, src_v, loc.at[0]),
        local(kw_in.at[0], kw.at[0], loc.at[1]),
        local(vw_in.at[0], vw.at[0], loc.at[2]),
        local(sgain, sg_v, loc.at[3]),
    ]
    target_load = [
        local(target.at[pl.ds(HALF * h, HALF)], xg.at[0, h, x], loc.at[(4, 9)[h]]) for h in (0, 1)
    ]
    def remote(src, dst, send, recv, device):
        pltpu.make_async_remote_copy(
            src_ref=src, dst_ref=dst, send_sem=send, recv_sem=recv,
            device_id=device, device_id_type=MESH,
        ).start()

    def await_bytes(ref, sem):
        pltpu.make_async_copy(ref, ref, sem).wait()

    def slot_of(fp, spos):
        return fp * 8 + spos

    for copy in first:
        copy.wait()
    second = [local(kw_in.at[1], kw.at[1], loc.at[7]), local(vw_in.at[1], vw.at[1], loc.at[8])]
    gains_load = local(tgains, tg_v, loc.at[5])
    q_load = local(qw_in, qw.at[c], loc.at[6])
    ff = dw_in.shape[1]
    late = [
        local(gw_in, raw.at[:, pl.ds(0, ff)], wts.at[0]),
        local(uw_in, raw.at[:, pl.ds(ff, ff)], wts.at[1]),
        local(dw_in, dn.at[c], wts.at[2]),
    ]
    own_rows = pl.ds(pl.multiple_of((c * 4 + x) * HD, HD), HD)
    own_out = [
        local(ow_in.at[l], ow.at[l, own_rows], own_sem.at[l]) for l in range(LAYERS)
    ]

    wide = src_v[...].astype(F32)
    scaled = wide * lax.rsqrt(jnp.mean(wide * wide, axis=-1, keepdims=True) + EPS)
    source_gains = sg_v[...].astype(F32)

    def project_source(l):
        normed = (scaled * source_gains[l : l + 1]).astype(BF)
        kv[l, slot_of(f, s), 0] = dot(normed, kw[l]).astype(BF)
        kv[l, slot_of(f, s), 1] = jnp.transpose(dot(normed, vw[l])).astype(BF)

    def send1(l, hop, way):
        delta = hop - 1
        fp = wrap(f - delta) if way == 0 else wrap(f + delta)
        block = kv.at[l, slot_of(fp, s)]
        if hop == 4:
            block = block.at[way]
        remote(block, block, kvs.at[l], r1.at[l, hop - 1, way], (ring1[way], tp))

    def recv1(l, hop, way):
        fp = wrap(f - hop) if way == 0 else wrap(f + hop)
        block = kv.at[l, slot_of(fp, s)]
        if hop == 4:
            block = block.at[way]
        await_bytes(block, r1.at[l, hop - 1, way])

    def send2(n, hop, way):
        l, k = divmod(n, 8)
        fp = wrap(f + ring_offset(k))
        delta = hop - 1
        spos = wrap(s - delta) if way == 0 else wrap(s + delta)
        block = kv.at[l, slot_of(fp, spos)]
        if hop == 4:
            block = block.at[way]
        remote(block, block, kvs.at[l], r2.at[n, hop - 1, way], (ring2[way], tp))

    def recv2(n, hop, way):
        l, k = divmod(n, 8)
        fp = wrap(f + ring_offset(k))
        spos = wrap(s - hop) if way == 0 else wrap(s + hop)
        block = kv.at[l, slot_of(fp, spos)]
        if hop == 4:
            block = block.at[way]
        await_bytes(block, r2.at[n, hop - 1, way])

    halves = {}
    waiting = []

    here, released = set(), set()

    def fresh(n):
        if n < 8 or (n in here and n in released):
            for w in (0, 1):
                send2(n, 1, w)

    def arrived(n):
        here.add(n)
        waiting.append((n // 8, n % 8, 0))
        fresh(n)

    def handle(event):
        ring, index, hop, way = event
        if ring == 3:
            released.add(index)
            fresh(index)
            return
        if ring == 0:
            for w in (0, 1):
                send1(index, 1, w)
            arrived(8 * index)
            return
        if hop == 4:
            halves[ring, index] = halves.get((ring, index), 0) + 1
        whole = hop < 4 or halves[ring, index] == 2
        if ring == 1:
            recv1(index, hop, way)
            if hop < 4:
                send1(index, hop + 1, way)
            if whole:
                arrived(8 * index + (2 * hop - way if hop < 4 else 7))
        else:
            recv2(index, hop, way)
            if hop < 4:
                send2(index, hop + 1, way)
            if whole:
                waiting.append((index // 8, index % 8, -hop if way == 0 else hop))

    groups = {0: [], 1: []}

    def attend(l, slots):
        done = groups[l]
        if slots is not None:
            keys = jnp.concatenate([kv[l, slot, 0] for slot in slots], axis=0)
            scores_ref[len(done) % 2] = dot(keys, qcat(l))
            done.append(slots)
        if len(done) == 1 and slots is not None:
            return
        past = -2 if slots is not None else -1
        values = jnp.concatenate([kv[l, slot, 1] for slot in done[past]], axis=1)
        scores = scores_ref[(len(done) + past) % 2]
        old = m_ref[...]
        new = jnp.maximum(old, jnp.max(scores, axis=0, keepdims=True))
        shrink = jnp.exp2(old - new)
        weights = jnp.exp2(scores - new)
        m_ref[...] = new
        l_ref[...] = l_ref[...] * shrink + jnp.sum(weights, axis=0, keepdims=True)
        acc_ref[...] = acc_ref[...] * shrink + dot(values, weights.astype(BF))

    def attend_waiting(l):
        blocks = [v for v in waiting if v[0] == l][:8]
        for v in blocks:
            waiting.remove(v)
        attend(l, [slot_of(wrap(f + ring_offset(k)), wrap(s + d)) for _, k, d in blocks])

    def qcat(l):
        return jnp.concatenate([qown[l], qrecv[l]], axis=1)

    def start_queries(l):
        gain = tg_v[l].astype(F32)[0:1]
        rows = xg[l].reshape(GROUP, D).astype(F32)
        normed = rms(rows, gain).astype(BF)
        theirs = dot(normed, qw[1 - c, l]) * QSCALE
        qsend[l] = jnp.transpose(theirs).astype(BF)
        remote(qsend.at[l], qrecv.at[l], q_send.at[l], q_recv.at[l], (sp, partner))
        mine = dot(normed, qw[c, l]) * QSCALE
        qown[l] = jnp.transpose(mine).astype(BF)
        m_ref[...] = jnp.full_like(m_ref, -1e30)
        l_ref[...] = jnp.zeros_like(l_ref)
        acc_ref[...] = jnp.zeros_like(acc_ref)

    def await_queries(l):
        await_bytes(qrecv.at[l], q_recv.at[l])

    def send_context(l):
        context = jnp.transpose(acc_ref[...] / l_ref[...]).astype(BF)
        slot = c * 4 + x
        csend[l] = context
        for h in (0, 1):
            mine = csend.at[l, pl.ds(h * PART, PART)]
            theirs = csend.at[l, pl.ds(GROUP + h * PART, PART)]
            here = cx.at[l, h, slot]
            for k in (2, 1, 3):
                chip = other_x(k) * 2
                remote(mine, here, c_send.at[l], c_recv.at[l, h], (sp, chip + c))
                remote(theirs, here, c_send.at[l], c_recv.at[l, h], (sp, chip + 1 - c))
            remote(theirs, here, c_send.at[l], c_recv.at[l, h], (sp, partner))
            cx[l, h, slot] = context[h * PART : (h + 1) * PART]

    def after_context(l, h):
        await_bytes(cx.at[l, h, pl.ds(0, 7)], c_recv.at[l, h])
        gains = tg_v[l].astype(F32)
        contexts = jnp.concatenate([cx[l, h, j] for j in range(8)], axis=1)
        attended = dot(contexts, ow[l]).astype(BF).astype(F32)
        rows = xg[l, h].reshape(PART, D).astype(F32)
        stream = (rows + rms(attended, gains[1:2])).astype(BF)
        mid[l, h] = stream.reshape(4, HALF, D)
        mixer_in = rms(stream.astype(F32), gains[2:3]).astype(BF)
        mixed = None
        for j in range(2):
            both = dot(mixer_in, gu[j, l])
            gate, up = both[:, :ff], both[:, ff:]
            hidden = (gate / (1.0 + jnp.exp(-gate)) * up).astype(BF)
            term = dot(hidden, dn[j, l])
            mixed = term if mixed is None else mixed + term
        rsend[l, h] = mixed.astype(BF).reshape(4, HALF, D)
        for k in (2, 1, 3):
            remote(
                rsend.at[l, h, other_x(k)], rs.at[l, h, x], s_send.at[l], s_recv.at[l, h],
                (sp, other_x(k) * 2 + c),
            )
        rs[l, h, x] = rsend[l, h, x]

    def after_sum(l, h):
        await_bytes(rs.at[l, h, pl.ds(0, 3)], s_recv.at[l, h])
        gain = tg_v[l].astype(F32)[3:4]
        total = rs[l, h, 0].astype(F32)
        for j in range(1, 4):
            total = total + rs[l, h, j].astype(F32)
        mixer_out = total.astype(BF).astype(F32)
        return mid[l, h, x].astype(F32) + rms(mixer_out, gain)

    def forward_out(l):
        own_out[l].wait()
        await_bytes(ow.at[l, pl.ds(0, 3 * HD)], o_recv.at[l])
        plane = pl.ds(pl.multiple_of(c * 512, 512), 512)
        remote(ow.at[l, plane], ow.at[l, plane], of_send.at[l], of_recv.at[l], (sp, partner))

    def send_target():
        for copy in target_load:
            copy.wait()
        for k in (2, 1, 3):
            remote(xg.at[0, :, x], xg.at[0, :, x], x_send.at[0], x_recv.at[0], (sp, other_x(k) * 2 + c))
        remote(qw_in, qw.at[c], pw_send.at[0], pw_recv.at[0], (sp, partner))

    def send_out(l):
        for k in (2, 1, 3):
            remote(
                ow_in.at[l], ow.at[l, own_rows], o_send.at[l], o_recv.at[l],
                (sp, other_x(k) * 2 + c),
            )

    def turn_ff():
        for copy in late:
            copy.wait()
        for l in range(LAYERS):
            gu[c, l] = jnp.transpose(raw[l])

    def send_ff():
        remote(gu.at[c], gu.at[c], pw_send.at[1], pw_recv.at[1], (sp, partner))
        remote(dw_in, dn.at[c], pw_send.at[2], pw_recv.at[2], (sp, partner))

    project_source(0)
    pl.semaphore_wait(barrier, len(peers))

    def begin_queries(l):
        if l == 0:
            gains_load.wait()
            q_load.wait()
            await_bytes(qw.at[0], pw_recv.at[0])
        await_bytes(xg.at[l, :, pl.ds(0, 3)], x_recv.at[l])
        start_queries(l)
        if l == 0:
            send_out(0)
            send_ff()

    def end_attention(l):
        attend(l, None)
        send_context(l)
        if l == 0:
            await_bytes(gu.at[0], pw_recv.at[1])
            await_bytes(dn.at[0], pw_recv.at[2])
        await_bytes(ow.at[l, pl.ds(0, 512)], of_recv.at[l])

    def next_rows(h):
        xg[1, h, x] = after_sum(0, h).astype(BF)
        for k in (2, 1, 3):
            remote(
                xg.at[1, h, x], xg.at[1, h, x], x_send.at[1], x_recv.at[1],
                (sp, other_x(k) * 2 + c),
            )

    def after_start():
        send_target()
        for copy in second:
            copy.wait()
        project_source(1)
        turn_ff()

    hooks = [(0.01, after_start), (15.0, lambda: send_out(1)), (23.0, lambda: forward_out(0)), (32.0, lambda: forward_out(1))]
    for when, task in plan(LATENCY, EXCHANGE, SWAP, RELEASES):
        while hooks and hooks[0][0] <= when:
            hooks.pop(0)[1]()
        kind, index, hop, _ = task
        if kind < 4:
            handle(task)
        elif kind == 4:
            begin_queries(index)
        elif kind == 5:
            await_queries(index)
        elif kind == 6:
            after_context(index, hop)
        elif kind == 7:
            next_rows(hop)
        elif kind == 8:
            attend_waiting(index)
        else:
            end_attention(index)
    after_context(1, 0)
    after_context(1, 1)
    for h in (0, 1):
        out[pl.ds(h * HALF, HALF)] = after_sum(1, h)

    for l in range(LAYERS):
        await_bytes(kv.at[l, pl.ds(0, 63)], kvs.at[l])
        await_bytes(xg.at[l, :, pl.ds(0, 3)], x_send.at[l])
        await_bytes(qsend.at[l], q_send.at[l])
        await_bytes(cx.at[l, :, pl.ds(0, 7)], c_send.at[l])
        await_bytes(rs.at[l, :, pl.ds(0, 3)], s_send.at[l])
        await_bytes(ow.at[l, pl.ds(0, 3 * HD)], o_send.at[l])
        await_bytes(ow.at[l, pl.ds(0, 512)], of_send.at[l])
    await_bytes(qw.at[0], pw_send.at[0])
    await_bytes(gu.at[0], pw_send.at[1])
    await_bytes(dn.at[0], pw_send.at[2])


def per_device(*args):
    args = list(args)
    ff = args[8].shape[2]
    args[8] = jnp.swapaxes(args[8], 1, 2)
    args[9] = jnp.swapaxes(args[9], 1, 2)
    hbm = pl.BlockSpec(memory_space=pl.ANY)
    vmem = pltpu.VMEM
    dma = pltpu.SemaphoreType.DMA
    scratch = [
        vmem((128, D), BF),
        vmem((LAYERS, 4, D), BF),
        vmem((LAYERS, D), BF),
        vmem((LAYERS, D, HD), BF),
        vmem((LAYERS, D, HD), BF),
        vmem((2, LAYERS, D, HD), BF),
        vmem((LAYERS, 2 * ff, D), BF),
        vmem((2, LAYERS, D, 2 * ff), BF),
        vmem((2, LAYERS, ff, D), BF),
        vmem((LAYERS, D, D), BF),
        vmem((LAYERS, BLOCKS, 2, HD, HD), BF),
        vmem((LAYERS, 2, 4, HALF, D), BF),
        vmem((LAYERS, HD, GROUP), BF),
        vmem((LAYERS, HD, GROUP), BF),
        vmem((LAYERS, HD, GROUP), BF),
        vmem((LAYERS, 2, 8, PART, HD), BF),
        vmem((LAYERS, 2 * GROUP, HD), BF),
        vmem((LAYERS, 2, 4, HALF, D), BF),
        vmem((LAYERS, 2, 4, HALF, D), BF),
        vmem((LAYERS, 2, 4, HALF, D), BF),
        vmem((1, 2 * GROUP), F32),
        vmem((1, 2 * GROUP), F32),
        vmem((HD, 2 * GROUP), F32),
        vmem((2, 8 * HD, 2 * GROUP), F32),
        dma((STEPS, 4, 2)),
        dma((LAYERS, 4, 2)),
        dma((LAYERS,)),
        dma((10,)),
        dma((3,)),
        dma((LAYERS,)),
    ]
    scratch += [dma((LAYERS,) + more) for more in ((), (), (), (), (2,), (), (2,), ())]
    scratch += [dma((3,)), dma((3,))]
    scratch += [dma((LAYERS,)) for _ in range(4)]
    wide = pl.pallas_call(
        kernel,
        out_shape=pltpu.VMEM((ROWS, D), F32),
        in_specs=[hbm] * 11,
        out_specs=pl.BlockSpec(memory_space=pltpu.VMEM),
        scratch_shapes=scratch,
        compiler_params=pltpu.CompilerParams(
            collective_id=0, has_side_effects=True, vmem_limit_bytes=60 * 1024 * 1024
        ),
    )(*args)
    return wide.astype(BF)


def solution(mesh):
    placed = (
        P(("sp", "tp"), None),
        P("sp", None),
        P(),
        P(),
        P(None, None, "tp"),
        P(None, None, "tp"),
        P(None, None, "tp"),
        P(None, "tp", None),
        P(None, None, "tp"),
        P(None, None, "tp"),
        P(None, "tp", None),
    )
    return jax.shard_map(
        per_device, mesh=mesh, in_specs=placed, out_specs=P(("sp", "tp"), None), check_vma=False
    )
```
